32 devices in a mesh: ep: 8 (over z, x), tp: 4 (over y, core).
Axes of the slice: x: 2, y: 2, z: 4, core: 2. Of those that a mesh axis runs over, the one named last changes fastest.
Arguments:
- tokens: bfloat16 [256, 2048], P('ep'), may hold values from -6 to 6
- lengths: int32 [256], P('ep'), may hold values from 128 to 1024, as said below
- cache_keys: bfloat16 [256, 1024, 1024], P('ep', None, 'tp'), may hold values from -140 to 140
- cache_values: bfloat16 [256, 1024, 1024], P('ep', None, 'tp'), may hold values from -6 to 6
- attn_gain: float32 [2048], replicated, may hold values from 0.1 to 1.9
- q_first_w: bfloat16 [2048, 512], P(None, 'tp'), may hold values from -0.19921875 to 0.19921875
- q_second_w: bfloat16 [2048, 512], P(None, 'tp'), may hold values from -0.19921875 to 0.19921875
- k_first_w: bfloat16 [2048, 512], P(None, 'tp'), may hold values from -0.125 to 0.125
- k_second_w: bfloat16 [2048, 512], P(None, 'tp'), may hold values from -0.125 to 0.125
- value_w: bfloat16 [2048, 1024], P(None, 'tp'), may hold values from -0.125 to 0.125
- mix_lambda: float32 [8], P('tp'), may hold values from 0.3 to 0.8
- head_gain: float32 [128], replicated, may hold values from 0.1 to 1.9
- out_w: bfloat16 [1024, 2048], P('tp'), may hold values from -0.09375 to 0.09375
- ffn_gain: float32 [2048], replicated, may hold values from 0.1 to 1.9
- routes: int32 [256, 4], P('ep'), may hold values from 0 to 31, all different within a row; in each aligned block of 32 rows (0 to 31, 32 to 63, ...) at most 8 rows name the same one
- route_logits: float32 [256, 4], P('ep'), may hold values from -4 to 4
- gate_w: bfloat16 [32, 2048, 1024], P('ep', None, 'tp'), may hold values from -0.34960938 to 0.34960938
- up_w: bfloat16 [32, 2048, 1024], P('ep', None, 'tp'), may hold values from -0.34960938 to 0.34960938
- down_w: bfloat16 [32, 1024, 2048], P('ep', None, 'tp'), may hold values from -0.125 to 0.125
Outputs:
- mixed: bfloat16 [256, 2048], P('ep', 'tp')
The draws below stay inside these ranges and needn't reach their ends.
Inputs may be any that keep to these rules, and one draw needn't show every extreme that they name: `lengths`: at least 128 positions; among the 32 sequences of each index of ep one holds exactly 1024. `routes`: each row names 4 different experts; within the rows of one device no expert is named more than 8 times, a bound that some block reaches.
All inputs are finite; a program needn't handle non-finite values.
Results may differ from the reference program's by a relative error of at most 0.015.
Values may be sent and summed in bfloat16 or wider, within the bound.
A program may use at most 128 MiB of HBM per device.

```python
import math
import jax
import jax.numpy as jnp
import numpy as np
from jax import lax

D = 2048
HEADS = 8
HEAD_DIM = 128
HALF = 64
FF = 1024
EXPERTS = 32
TOP = 4
SEQ_GRP = 32
CACHE = 1024
SEQS = 256
CAP = 8
N_EP = 8


def draw_tokens(key, part):
    column = jnp.arange(D, dtype=jnp.float32) / max(D - 1, 1)
    col_scale = jnp.exp(jnp.log(0.2) + jnp.log(10.0) * column)[None, :]
    noise = jnp.clip(jax.random.normal(key, (SEQS, D), jnp.float32), -3.0, 3.0)
    return (noise * col_scale).astype(jnp.bfloat16)


def draw_lengths(key, part):
    lowest = max(4, CACHE // 8)
    spread = jax.random.randint(key, (SEQS,), lowest, CACHE + 1)
    groups = SEQS // SEQ_GRP
    picks = jax.random.randint(jax.random.fold_in(key, 7), (groups,), 0, SEQ_GRP)
    places = jnp.arange(SEQS, dtype=jnp.int32)
    longest = places % SEQ_GRP == jnp.repeat(picks, SEQ_GRP)
    return jnp.where(longest, CACHE, spread).astype(jnp.int32)


def draw_cache_keys(key, part):
    width = HEADS * HEAD_DIM
    noise = jnp.clip(jax.random.normal(key, (SEQS, CACHE, width), jnp.float32), -5.0, 5.0)
    return noise.astype(jnp.bfloat16)


def block_levels(key, dims, pieces, least, top_value):
    loudness = 1.0
    for dim, shards_of in pieces:
        draws = jax.random.uniform(jax.random.fold_in(jax.random.fold_in(key, 6), dim), (shards_of,), jnp.float32, least / len(pieces), top_value / len(pieces))
        loudness = loudness * jnp.repeat(jnp.exp(draws), dims[dim] // shards_of).reshape((-1,) + (1,) * (len(dims) - 1 - dim))
    return loudness


def deal_out(stream_key, own, number, rows, amount, top, most, lean):
    order = jax.random.permutation(stream_key, amount)
    heavy_load, usual = load_shares(amount, rows * top, most, lean, True), load_shares(amount, rows * top, most, lean, False)
    places = jnp.arange(amount)

    def named(sizes, turn):
        used = int((sizes > 0).sum())
        fixed = max(1, used // 4)
        moved = fixed + (places - fixed + turn * (used - fixed)) % max(1, amount - fixed)
        return jnp.zeros((amount,), jnp.int32).at[order[jnp.where(places < fixed, places, moved)]].set(jnp.asarray(sizes, jnp.int32))

    sizes = jnp.where(number % 4 == 0, named(heavy_load, number // 4), named(usual, number - number // 4 - 1))
    mixed = jax.random.permutation(jax.random.fold_in(own, 3), amount)
    source_of, sink = mixed[0:amount // 2 * 2:2], mixed[1:amount // 2 * 2:2]
    room = jnp.minimum(sizes[source_of] - 1, most - sizes[sink]) // 2
    room = jnp.where((source_of == order[0]) | (sink == order[0]) | (sizes[sink] == 0), 0, jnp.maximum(room, 0))
    moved = jax.random.randint(jax.random.fold_in(own, 4), (amount // 2,), 0, 1 << 20) % (room + 1)
    sizes = sizes.at[source_of].add(-moved).at[sink].add(moved)
    members = jnp.searchsorted(jnp.cumsum(sizes), jnp.arange(rows * top), side="right").astype(jnp.int32)
    grid = members.reshape(top, rows).T
    grid = grid[jax.random.permutation(jax.random.fold_in(own, 1), rows)]
    turn = jax.random.randint(jax.random.fold_in(own, 2), (rows, 1), 0, top)
    return jnp.take_along_axis(grid, (jnp.arange(top)[None, :] + turn) % top, axis=1)


def load_shares(amount, total, limit, lean, full):
    loads = [(1 << 20) // math.isqrt(grade ** lean) + 1 for grade in range(1, amount + 1)]
    largest = limit if full else min(limit, max(-(-total // amount), total * loads[0] // sum(loads)))
    least = 1 if total - largest >= amount - 1 else 0
    given, surplus = [largest] + [least] * (amount - 1), total - largest - least * (amount - 1)
    while surplus > 0:
        free = [i for i in range(1, amount) if given[i] < largest] or [i for i in range(1, amount) if given[i] < limit]
        pool, budget = sum([loads[i] for i in free]), surplus
        for i in free:
            addition = min(limit - given[i], max(1, budget * loads[i] // pool), surplus)
            given[i] = given[i] + addition
            surplus = surplus - addition
    return np.array(given)


def bell_draw(rng, extent, scale, limit, pieces=(), held_as=jnp.bfloat16):
    factor_of = block_levels(rng, extent, pieces, -0.22, 0.18) if pieces else 1.0
    result = jax.random.normal(rng, extent, jnp.float32) * scale * factor_of
    return jnp.minimum(jnp.maximum(result, -limit), limit).astype(held_as)


def setup_inputs(seed: int = 0) -> dict:
    key_list = jax.random.split(jax.random.key(seed), 20)
    tokens = draw_tokens(jax.random.fold_in(key_list[19], 71), 0)
    lengths = draw_lengths(jax.random.fold_in(key_list[19], 71), 0)
    cache_keys = draw_cache_keys(jax.random.fold_in(key_list[19], 71), 0)
    cache_values = bell_draw(key_list[3], (SEQS, CACHE, HEADS * HEAD_DIM), 1.0, 6.0, ((0, 8), (2, 4)))
    attn_gain = jnp.clip(1.0 + 0.18 * jax.random.normal(key_list[4], (D,), jnp.float32), 0.1, 1.9)
    q_first_w = bell_draw(key_list[5], (D, HEADS * HALF), 0.0387, 0.19921875, ((1, 4),))
    q_second_w = bell_draw(key_list[6], (D, HEADS * HALF), 0.0387, 0.19921875, ((1, 4),))
    k_first_w = bell_draw(key_list[7], (D, HEADS * HALF), D ** -0.5, 0.125, ((1, 4),))
    k_second_w = bell_draw(key_list[8], (D, HEADS * HALF), D ** -0.5, 0.125, ((1, 4),))
    value_w = bell_draw(key_list[9], (D, HEADS * HEAD_DIM), D ** -0.5, 0.125, ((1, 4),))
    mix_lambda = jnp.clip(0.3 + 0.5 * jax.random.uniform(key_list[10], (HEADS,), jnp.float32) ** block_levels(key_list[10], (HEADS,), ((0, 4),), -0.2, 0.2), 0.3, 0.8)
    head_gain = jnp.clip(1.0 + 0.18 * jax.random.normal(key_list[11], (HEAD_DIM,), jnp.float32), 0.1, 1.9)
    out_w = bell_draw(key_list[12], (HEADS * HEAD_DIM, D), (0.5 * (HEADS * HEAD_DIM) ** -0.5), 0.09375, ((0, 4),))
    ffn_gain = jnp.clip(1.0 + 0.18 * jax.random.normal(key_list[13], (D,), jnp.float32), 0.1, 1.9)
    routes_keys = jax.random.split(jax.random.fold_in(key_list[14], 1), SEQS // SEQ_GRP)
    routes_turns = jax.random.permutation(jax.random.fold_in(key_list[14], 3), SEQS // SEQ_GRP)
    routes = jax.vmap(lambda own, number: deal_out(jax.random.fold_in(key_list[14], 2), own, number, SEQ_GRP, EXPERTS, TOP, CAP, 2))(routes_keys, routes_turns).reshape((SEQS, TOP))
    route_logits = bell_draw(key_list[15], (SEQS, TOP), 1.0, 4.0, ((0, 8),), jnp.float32)
    gate_w = bell_draw(key_list[16], (EXPERTS, D, FF), 0.066, 0.34960938, ((0, 8), (2, 4)))
    up_w = bell_draw(key_list[17], (EXPERTS, D, FF), 0.066, 0.34960938, ((0, 8), (2, 4)))
    down_w = bell_draw(key_list[18], (EXPERTS, FF, D), (2 * FF) ** -0.5, 0.125, ((0, 8), (2, 4)))
    return {"tokens": tokens, "lengths": lengths, "cache_keys": cache_keys, "cache_values": cache_values, "attn_gain": attn_gain, "q_first_w": q_first_w, "q_second_w": q_second_w, "k_first_w": k_first_w, "k_second_w": k_second_w, "value_w": value_w, "mix_lambda": mix_lambda, "head_gain": head_gain, "out_w": out_w, "ffn_gain": ffn_gain, "routes": routes, "route_logits": route_logits, "gate_w": gate_w, "up_w": up_w, "down_w": down_w}


EPS = 1e-06
LIMIT = 7.0
ALPHA = 1.702

def rms_scale(rows, gain):
    mean_sq = lax.optimization_barrier(jnp.mean(rows * rows, axis=-1, keepdims=True))
    return rows * lax.rsqrt(mean_sq + EPS) * gain

def slot_tables(routes, weights, expert_ids, capacity):
    blocks, seqs, top = routes.shape
    flat = routes.reshape(blocks, seqs * top)
    order = jnp.arange(seqs * top, dtype=jnp.int32)
    same = (flat[:, None, :] == flat[:, :, None]) & (order[None, None, :] < order[None, :, None])
    rank = lax.optimization_barrier(jnp.sum(same.astype(jnp.int32), axis=2))
    match = flat[:, :, None] == expert_ids[None, None, :]
    hit = rank[:, :, None] == jnp.arange(capacity, dtype=jnp.int32)[None, None, :]
    table = (match[:, :, :, None] & hit[:, :, None, :]).astype(jnp.float32)
    table = table.reshape(blocks, seqs, top, expert_ids.shape[0], capacity)
    dispatch = lax.optimization_barrier(jnp.sum(table, axis=2))
    combine = lax.optimization_barrier(jnp.sum(table * weights[:, :, :, None, None], axis=2))
    return (dispatch, combine)

def reference(tokens, lengths, cache_keys, cache_values, attn_gain, q_first_w, q_second_w, k_first_w, k_second_w, value_w, mix_lambda, head_gain, out_w, ffn_gain, routes, route_logits, gate_w, up_w, down_w):
    wide = tokens.astype(jnp.float32)
    normed = rms_scale(wide, attn_gain).astype(jnp.bfloat16)
    seqs = tokens.shape[0]
    half = HEAD_DIM // 2
    scale = half ** (-0.5)

    def project(weight, size):
        return jnp.dot(normed, weight, preferred_element_type=jnp.float32).astype(jnp.bfloat16).reshape(seqs, HEADS, size)
    q_first = project(q_first_w, half)
    q_second = project(q_second_w, half)
    k_first = project(k_first_w, half)
    k_second = project(k_second_w, half)
    new_value = project(value_w, HEAD_DIM)
    valid = jnp.arange(CACHE, dtype=jnp.int32)[None, :] < lengths[:, None]
    outputs = []
    for head in range(HEADS):
        keys = cache_keys[:, :, head * HEAD_DIM:(head + 1) * HEAD_DIM].astype(jnp.float32)
        values = cache_values[:, :, head * HEAD_DIM:(head + 1) * HEAD_DIM].astype(jnp.float32)
        maps = []
        for query, own_key, start in ((q_first, k_first, 0), (q_second, k_second, half)):
            query_f = query[:, head].astype(jnp.float32)
            own_f = own_key[:, head].astype(jnp.float32)
            scores = jnp.einsum('sd,std->st', query_f, keys[:, :, start:start + half]) * scale
            own = lax.optimization_barrier(jnp.sum(query_f * own_f, axis=-1)) * scale
            scores = jnp.where(valid, scores, -jnp.inf)
            top = jnp.maximum(lax.optimization_barrier(jnp.max(scores, axis=-1)), own)
            raised = jnp.exp(scores - top[:, None])
            own_raised = jnp.exp(own - top)
            total = lax.optimization_barrier(jnp.sum(raised, axis=-1)) + own_raised
            maps.append((raised / total[:, None], own_raised / total))
        lam = mix_lambda[head]
        mixed_w = (maps[0][0] - lam * maps[1][0]).astype(jnp.bfloat16)
        own_w = (maps[0][1] - lam * maps[1][1]).astype(jnp.bfloat16)
        head_out = jnp.einsum('st,std->sd', mixed_w.astype(jnp.float32), values)
        head_out = head_out + own_w.astype(jnp.float32)[:, None] * new_value[:, head].astype(jnp.float32)
        outputs.append(rms_scale(head_out, head_gain).astype(jnp.bfloat16))
    attended = jnp.stack(outputs, axis=1).reshape(seqs, HEADS * HEAD_DIM)
    after = wide + jnp.dot(attended, out_w, preferred_element_type=jnp.float32)
    expert_in = rms_scale(after, ffn_gain).astype(jnp.bfloat16)
    weights = jax.nn.softmax(route_logits, axis=-1)
    dispatch, combine = slot_tables(routes.reshape(N_EP, SEQ_GRP, TOP), weights.reshape(N_EP, SEQ_GRP, TOP), jnp.arange(EXPERTS, dtype=jnp.int32), CAP)
    buffer = jnp.einsum('bsec,bsd->becd', dispatch, expert_in.reshape(N_EP, SEQ_GRP, D).astype(jnp.float32)).astype(jnp.bfloat16)
    stacked = jnp.transpose(buffer, (1, 0, 2, 3)).reshape(EXPERTS, N_EP * CAP, D)

    def one_expert(items):
        rows, w_gate, w_up, w_down = items
        gate = jnp.dot(rows, w_gate, preferred_element_type=jnp.float32)
        up = jnp.dot(rows, w_up, preferred_element_type=jnp.float32)
        bound_gate = jnp.minimum(gate, LIMIT)
        bound_up = jnp.clip(up, -LIMIT, LIMIT)
        hidden = ((bound_up + 1.0) * bound_gate * jax.nn.sigmoid(ALPHA * bound_gate)).astype(jnp.bfloat16)
        return jnp.dot(hidden, w_down, preferred_element_type=jnp.float32).astype(jnp.bfloat16)
    results = lax.map(one_expert, (stacked, gate_w, up_w, down_w)).reshape(EXPERTS, N_EP, CAP, D)
    moe = jnp.einsum('bsec,ebcd->bsd', combine, results.astype(jnp.float32), precision=lax.Precision.HIGHEST).reshape(seqs, D)
    return (after + moe).astype(jnp.bfloat16)
```

```python
import functools

import jax
import jax.numpy as jnp
from jax import lax
from jax.experimental import pallas as pl
from jax.experimental.pallas import tpu as pltpu
from jax.sharding import PartitionSpec as P

EPS = 1e-06
LIMIT = 7.0
ALPHA = 1.702
PIECE = 128
GROUP = 8
VMEM_BYTES = 67043328
F32 = jnp.float32
BF16 = jnp.bfloat16


def attend_kernel(
    heads,
    lam_ref,
    lengths_hbm,
    tokens_hbm,
    again_hbm,
    hgain_hbm,
    keys_hbm,
    values_hbm,
    q1_hbm,
    q2_hbm,
    k1_hbm,
    k2_hbm,
    vw_hbm,
    ow_hbm,
    part_ref,
    kbuf,
    vbuf,
    q1_v,
    q2_v,
    k1_v,
    k2_v,
    vw_v,
    ow_v,
    queries,
    own_keys,
    new_values,
    attended,
    raw,
    weights_v,
    lengths_ref,
    tokens_ref,
    again_ref,
    hgain_ref,
    ksem,
    vsem,
    wsem,
    ssem,
):
    smalls = ((lengths_hbm, lengths_ref), (tokens_hbm, tokens_ref), (again_hbm, again_ref), (hgain_hbm, hgain_ref))
    smalls = [pltpu.make_async_copy(src, dst, ssem.at[i]) for i, (src, dst) in enumerate(smalls)]
    for small in smalls:
        small.start()
    seqs, length, width = kbuf.shape
    head = width // heads
    half = head // 2
    scale = half ** (-0.5)
    weights = ((q1_hbm, q1_v), (q2_hbm, q2_v), (k1_hbm, k1_v), (k2_hbm, k2_v), (vw_hbm, vw_v), (ow_hbm, ow_v))
    loads = [pltpu.make_async_copy(src, dst, wsem.at[i]) for i, (src, dst) in enumerate(weights)]
    for load in loads[:5]:
        load.start()

    def fetch(s):
        rows = pl.multiple_of((lengths_ref[s] + (PIECE - 1)) // PIECE * PIECE, PIECE)
        return (
            pltpu.make_async_copy(keys_hbm.at[s, pl.ds(0, rows)], kbuf.at[s, pl.ds(0, rows)], ksem.at[s]),
            pltpu.make_async_copy(values_hbm.at[s, pl.ds(0, rows)], vbuf.at[s, pl.ds(0, rows)], vsem.at[s]),
        )

    def start(s, carry):
        a, b = fetch(s)
        a.start()
        b.start()
        return carry

    smalls[0].wait()
    lax.fori_loop(0, seqs, start, 0)
    loads[5].start()
    for small in smalls[1:]:
        small.wait()

    wide = tokens_ref[...].astype(F32)
    normed = (
        wide * lax.rsqrt(jnp.mean(wide * wide, axis=-1, keepdims=True) + EPS) * again_ref[...]
    ).astype(BF16)
    for load in loads[:5]:
        load.wait()

    def project(w):
        return jnp.dot(normed, w[...], preferred_element_type=F32).astype(BF16).astype(F32)

    q1, q2, k1, k2 = project(q1_v), project(q2_v), project(k1_v), project(k2_v)
    new_values[...] = project(vw_v)
    zero = jnp.zeros((seqs, half), F32)
    queries[...] = jnp.zeros_like(queries)
    kparts = []
    for h in range(heads):
        cut = slice(h * half, (h + 1) * half)
        kparts += [k1[:, cut], k2[:, cut]]
        for p, q in ((0, q1), (1, q2)):
            parts = [zero] * (2 * heads)
            parts[2 * h + p] = q[:, cut]
            queries[:, 4 * p + h, :] = jnp.concatenate(parts, axis=-1)
    own_keys[...] = jnp.concatenate(kparts, axis=-1)

    position = lax.broadcasted_iota(jnp.int32, (8, length), 1)
    row = lax.broadcasted_iota(jnp.int32, (8, width), 0)
    mine = row == lax.broadcasted_iota(jnp.int32, (8, width), 1) // head
    map_row = lax.broadcasted_iota(jnp.int32, (8, 1), 0)
    lam = jnp.zeros((8, 1), F32)
    for h in range(heads):
        lam = jnp.where(map_row == h, lam_ref[h], lam)
    hgain = jnp.concatenate([hgain_ref[...]] * heads, axis=-1)

    def group_step(g, carry):
        for j in range(GROUP):
            for copy in fetch(g * GROUP + j):
                copy.wait()
        for j in range(GROUP):
            s = g * GROUP + j
            raw[j] = lax.dot_general(
                queries[s].astype(BF16), kbuf[s], (((1,), (1,)), ((), ())), preferred_element_type=F32
            )
        own_ws = []
        for j in range(GROUP):
            s = g * GROUP + j
            own = jnp.sum(queries[s] * own_keys[pl.ds(s, 1), :], axis=-1, keepdims=True) * scale
            scores = jnp.where(position < lengths_ref[s], raw[j] * scale, -jnp.inf)
            top = jnp.maximum(jnp.max(scores, axis=-1, keepdims=True), own)
            raised = jnp.exp(scores - top)
            own_raised = jnp.exp(own - top)
            total = jnp.sum(raised, axis=-1, keepdims=True) + own_raised
            inv = 1.0 / total
            probs = raised * inv
            own_probs = own_raised * inv
            weights_v[j] = (probs - lam * pltpu.roll(probs, 4, 0)).astype(BF16)
            own_b = jnp.broadcast_to(own_probs, (8, 128))
            own_ws.append((own_b - lam * pltpu.roll(own_b, 4, 0)).astype(BF16).astype(F32)[:, :1])
        outs = []
        for j in range(GROUP):
            s = g * GROUP + j
            count = lengths_ref[s]
            pieces = [
                jnp.where(c * PIECE < count, vbuf[s, c * PIECE:(c + 1) * PIECE, :], jnp.zeros((PIECE, width), BF16))
                for c in range(length // PIECE)
            ]
            outs.append(jnp.dot(weights_v[j], jnp.concatenate(pieces, axis=0), preferred_element_type=F32))
        for j in range(GROUP):
            s = g * GROUP + j
            out = outs[j] + own_ws[j] * new_values[pl.ds(s, 1), :]
            out = jnp.where(mine, out, 0.0)
            mean_sq = jnp.sum(out * out, axis=-1, keepdims=True) * (1.0 / head)
            out = out * lax.rsqrt(mean_sq + EPS)
            attended[pl.ds(s, 1), :] = jnp.sum(out, axis=0, keepdims=True) * hgain
        return carry

    lax.fori_loop(0, seqs // GROUP, group_step, 0)
    loads[5].wait()
    part_ref[...] = jnp.dot(
        attended[...].astype(BF16), ow_v[...], preferred_element_type=F32
    ).reshape(part_ref.shape).astype(part_ref.dtype)


def attend(
    tokens, lengths, cache_keys, cache_values, attn_gain, q1w, q2w, k1w, k2w, vw, lam, hgain, out_w, out_dtype, parts
):
    seqs, length, width = cache_keys.shape
    heads = lam.shape[0]
    vm = pl.BlockSpec(memory_space=pltpu.VMEM)
    anyspace = pl.BlockSpec(memory_space=pltpu.HBM)
    scratch = [pltpu.VMEM(cache_keys.shape, BF16), pltpu.VMEM(cache_values.shape, BF16)]
    scratch += [pltpu.VMEM(w.shape, BF16) for w in (q1w, q2w, k1w, k2w, vw, out_w)]
    scratch += [
        pltpu.VMEM((seqs, 8, width), F32),
        pltpu.VMEM((seqs, width), F32),
        pltpu.VMEM((seqs, width), F32),
        pltpu.VMEM((seqs, width), F32),
        pltpu.VMEM((GROUP, 8, length), F32),
        pltpu.VMEM((GROUP, 8, length), BF16),
        pltpu.SMEM((seqs,), jnp.int32),
        pltpu.VMEM(tokens.shape, BF16),
        pltpu.VMEM((1, tokens.shape[1]), F32),
        pltpu.VMEM((1, hgain.shape[0]), F32),
        pltpu.SemaphoreType.DMA((seqs,)),
        pltpu.SemaphoreType.DMA((seqs,)),
        pltpu.SemaphoreType.DMA((6,)),
        pltpu.SemaphoreType.DMA((4,)),
    ]
    return pl.pallas_call(
        functools.partial(attend_kernel, heads),
        out_shape=jax.ShapeDtypeStruct((parts, seqs // parts, out_w.shape[1]), out_dtype),
        in_specs=[pl.BlockSpec(memory_space=pltpu.SMEM)] + [anyspace] * 12,
        out_specs=vm,
        scratch_shapes=scratch,
        compiler_params=pltpu.CompilerParams(vmem_limit_bytes=VMEM_BYTES),
        name="attend",
    )(
        lam, lengths, tokens, attn_gain.reshape(1, -1), hgain.reshape(1, -1),
        cache_keys, cache_values, q1w, q2w, k1w, k2w, vw, out_w,
    )


MESH = pl.DeviceIdType.MESH


def rms_scale(rows, gain):
    mean_sq = jnp.mean(rows * rows, axis=-1, keepdims=True)
    return rows * lax.rsqrt(mean_sq + EPS) * gain


def exact_dot(a, b):
    return jnp.dot(a, b, precision=lax.Precision.HIGHEST, preferred_element_type=F32)


def where_is(shape, dim):
    return lax.broadcasted_iota(jnp.int32, shape, dim)


def turned_dot(a, b, left, right):
    return lax.dot_general(
        a, b, (((left,), (right,)), ((), ())), precision=lax.Precision.HIGHEST, preferred_element_type=F32
    )


def route_tables(routes, logits, slots, capacity):
    top, seqs = routes.shape
    n = seqs * top
    routes = routes.astype(F32)
    spread = turned_dot(routes, (where_is((top, n), 1) % top == where_is((top, n), 0)).astype(F32), 0, 0)
    row = jnp.sum(jnp.where(where_is((seqs, n), 1) // top == where_is((seqs, n), 0), spread, 0.0), axis=0, keepdims=True)
    owner = (where_is((n, seqs), 0) // top == where_is((n, seqs), 1)).astype(F32)
    pick = where_is((n, top), 0) % top == where_is((n, top), 1)
    col = jnp.sum(jnp.where(pick, turned_dot(owner, routes, 1, 1), 0.0), axis=1, keepdims=True)
    same = row == col
    i, j = where_is((n, n), 0), where_is((n, n), 1)
    rank_col = jnp.sum((same & (j < i)).astype(F32), axis=1, keepdims=True)
    rank_row = jnp.sum((same & (i < j)).astype(F32), axis=0, keepdims=True)
    slot_row = row * capacity + rank_row
    return slot_row, lambda: combine_table(logits, col, rank_col, owner, pick, slots, capacity)


def combine_table(logits, col, rank_col, owner, pick, slots, capacity):
    n, seqs = owner.shape
    top = n // seqs
    slot_col = col * capacity + rank_col
    raised = jnp.exp(logits - jnp.max(logits, axis=0, keepdims=True))
    weights = raised / jnp.sum(raised, axis=0, keepdims=True)
    weight_col = jnp.sum(jnp.where(pick, turned_dot(owner, weights, 1, 1), 0.0), axis=1, keepdims=True)
    hit = where_is((n, slots), 1).astype(F32) == slot_col
    member = (where_is((seqs, n), 1) // top == where_is((seqs, n), 0)).astype(F32)
    combine = exact_dot(member, jnp.where(hit, weight_col, 0.0))
    return combine


def experts_kernel(
    groups,
    parts,
    capacity,
    part_ref,
    tokens_ref,
    fgain_ref,
    routes_ref,
    logits_ref,
    gate_hbm,
    up_hbm,
    down_hbm,
    out_ref,
    gate_v,
    up_v,
    down_v,
    rs_buf,
    wide,
    after,
    kept,
    slot_buf,
    xbuf,
    hbuf,
    resbuf,
    ret,
    combine_v,
    wsem,
    rs_s,
    rs_r,
    sl_s,
    sl_r,
    k_s,
    k_r,
    xe_s,
    xe_r,
    xy_s,
    xy_r,
    xc_s,
    xc_r,
    xd_s,
    xd_r,
    hy_s,
    hy_r,
    hc_s,
    hc_r,
    hd_s,
    hd_r,
    re_s,
    re_r,
):
    e, t = lax.axis_index("ep"), lax.axis_index("tp")
    owned = gate_v.shape[0]
    rows, width = after.shape
    columns = out_ref.shape[1]
    seqs = rows * parts
    top = routes_ref.shape[0]
    n = seqs * top
    block = owned * capacity
    twin = t + 1 - 2 * lax.rem(t, 2)
    across = lax.rem(t + 2, parts)

    loads = []
    for j in range(owned):
        for i, (src, dst) in enumerate(((gate_hbm, gate_v), (up_hbm, up_v), (down_hbm, down_v))):
            loads.append(pltpu.make_async_copy(src.at[j], dst.at[j], wsem.at[3 * j + i]))
            loads[-1].start()

    barrier = pltpu.get_barrier_semaphore()
    for k in range(1, parts):
        pl.semaphore_signal(barrier, inc=1, device_id=(e, lax.rem(t + k, parts)), device_id_type=MESH)
    for k in range(1, groups):
        pl.semaphore_signal(barrier, inc=1, device_id=(lax.rem(e + k, groups), t), device_id_type=MESH)
    pl.semaphore_wait(barrier, parts + groups - 2)

    sent = []

    def send(src, dst, s_sem, r_sem, device):
        copy = pltpu.make_async_remote_copy(
            src_ref=src, dst_ref=dst, send_sem=s_sem, recv_sem=r_sem, device_id=device, device_id_type=MESH
        )
        copy.start()
        sent.append(copy)
        return copy

    scatter = []
    for k in range(1, parts):
        peer = lax.rem(t + k, parts)
        scatter.append(send(part_ref.at[peer], rs_buf.at[k - 1], rs_s.at[k - 1], rs_r.at[k - 1], (e, peer)))

    slot_row, later = route_tables(routes_ref[...], logits_ref[...], groups * block, capacity)
    slot_buf[e] = jnp.broadcast_to(slot_row, (8, n))
    tables = []
    for k in range(1, groups):
        tables.append(
            send(slot_buf.at[e], slot_buf.at[e], sl_s.at[k - 1], sl_r.at[k - 1], (lax.rem(e + k, groups), t))
        )
    wide[...] = tokens_ref[...].astype(F32).reshape(parts, rows, width)
    total = part_ref[t].astype(F32)
    for k in range(1, parts):
        scatter[k - 1].wait_recv()
        total = total + rs_buf[k - 1].astype(F32)
    total = wide[t] + total
    after[...] = total
    xbuf[e, t] = rms_scale(total, fgain_ref[...]).astype(BF16)

    inner = 2 if groups % 2 == 0 else 1
    outer = groups // inner
    place_out, place_in = e // inner, lax.rem(e, inner)
    gather = []
    for m in range(1, outer):
        peer = lax.rem(place_out + m, outer) * inner + place_in
        gather.append(send(xbuf.at[e, t], xbuf.at[e, t], xe_s.at[m - 1], xe_r.at[m - 1], (peer, t)))
    side = place_out * inner + inner - 1 - place_in
    turns = [(0, 0)]
    for m in range(1, outer):
        turns += [(m, 0)] + [(m - 1, 1)] * (inner - 1)
    turns += [(outer - 1, 1)] * (inner - 1)
    passed = [None] * outer
    sources = []
    far, near, relay = [], [], []
    for k, (m, other) in enumerate(turns):
        line_in = inner - 1 - place_in if other else place_in
        source = lax.rem(place_out - m + outer, outer) * inner + line_in
        sources.append(source)
        if other:
            passed[m].wait_recv()
        elif m:
            gather[m - 1].wait_recv()
        if inner > 1 and not other:
            i = outer - 1 + m
            passed[m] = send(xbuf.at[source, t], xbuf.at[source, t], xe_s.at[i], xe_r.at[i], (side, t))
        mine = xbuf.at[source, t]
        far.append(send(mine, mine, xy_s.at[k], xy_r.at[k], (e, across)))
        near.append(send(mine, mine, xc_s.at[k], xc_r.at[k], (e, twin)))
        if k == 0:
            combine_v[...] = later()
            keep = []
            kept[t] = after[:, pl.ds(pl.multiple_of(t * columns, columns), columns)]
            for q in range(1, parts):
                peer = lax.rem(t + q, parts)
                view = after.at[:, pl.ds(pl.multiple_of(peer * columns, columns), columns)]
                keep.append(send(view, kept.at[t], k_s.at[q - 1], k_r.at[q - 1], (e, peer)))
    for table in tables:
        table.wait_recv()
    base = e * block
    local = (where_is((block, n), 0) + base).astype(F32)
    place = []
    for b in range(groups):
        chosen = (slot_buf[b][:1, :] == local).astype(BF16)
        spot = (where_is((n, groups * seqs), 1) == where_is((n, groups * seqs), 0) // top + b * seqs).astype(BF16)
        placed = jnp.dot(chosen, spot, preferred_element_type=F32)
        place.append(placed.reshape(owned, 1, capacity, groups * seqs))
    dispatch = jnp.concatenate(place, axis=1).reshape(groups * block, groups * seqs).astype(BF16)
    for k, source in enumerate(sources):
        far[k].wait_recv()
        theirs = xbuf.at[source, across]
        relay.append(send(theirs, theirs, xd_s.at[k], xd_r.at[k], (e, twin)))
    for copy in near + relay:
        copy.wait_recv()

    everything = xbuf[...].astype(F32).reshape(groups * seqs, width).astype(BF16)
    lines = jnp.dot(dispatch, everything, preferred_element_type=F32).astype(BF16)
    per = groups * capacity
    hfar, hnear = [], []
    for j in range(owned):
        for i in range(2):
            loads[3 * j + i].wait()
        line = lines[j * per:(j + 1) * per]
        gate = jnp.minimum(jnp.dot(line, gate_v[j], preferred_element_type=F32), LIMIT)
        up = jnp.clip(jnp.dot(line, up_v[j], preferred_element_type=F32), -LIMIT, LIMIT)
        hbuf[j, t] = ((up + 1.0) * gate * jax.nn.sigmoid(ALPHA * gate)).astype(BF16)
        mine = hbuf.at[j, t]
        hfar.append(send(mine, mine, hy_s.at[j], hy_r.at[j], (e, across)))
        hnear.append(send(mine, mine, hc_s.at[j], hc_r.at[j], (e, twin)))
    deep = hbuf.shape[3]
    hrelay, back = [], []
    for j in range(owned + 1):
        if j < owned:
            hfar[j].wait_recv()
            theirs = hbuf.at[j, across]
            hrelay.append(send(theirs, theirs, hd_s.at[j], hd_r.at[j], (e, twin)))
        if j == 0:
            continue
        i = j - 1
        hnear[i].wait_recv()
        hrelay[i].wait_recv()
        loads[3 * i + 2].wait()
        result = jnp.zeros((per, columns), F32)
        for q in range(parts):
            result += jnp.dot(hbuf[i, q], down_v[i, q * deep:(q + 1) * deep, :], preferred_element_type=F32)
        resbuf[i] = result.reshape(groups, capacity, columns).astype(BF16)
        for k in range(1, groups):
            peer = lax.rem(e + k, groups)
            n_back = i * (groups - 1) + k - 1
            back.append(send(resbuf.at[i, peer], ret.at[e, i], re_s.at[n_back], re_r.at[n_back], (peer, t)))
        ret[e, i] = resbuf[i, e]
    for copy in keep + back:
        copy.wait_recv()
    moe = exact_dot(combine_v[...], ret[...].astype(F32).reshape(groups * block, columns))
    out_ref[...] = (kept[...].reshape(seqs, columns) + moe).astype(out_ref.dtype)
    for copy in sent:
        copy.wait_send()


def experts(part, tokens, ffn_gain, routes, logits, gate_w, up_w, down_w, groups, parts, capacity):
    seqs, width = tokens.shape
    rows = seqs // parts
    owned, _, deep = gate_w.shape
    columns = down_w.shape[2]
    per = groups * capacity
    vm = pl.BlockSpec(memory_space=pltpu.VMEM)
    anyspace = pl.BlockSpec(memory_space=pltpu.HBM)
    dma = lambda count: [pltpu.SemaphoreType.DMA((count,)), pltpu.SemaphoreType.DMA((count,))]
    scratch = [
        pltpu.VMEM(gate_w.shape, BF16),
        pltpu.VMEM(up_w.shape, BF16),
        pltpu.VMEM(down_w.shape, BF16),
        pltpu.VMEM((parts - 1, rows, width), BF16),
        pltpu.VMEM((parts, rows, width), F32),
        pltpu.VMEM((rows, width), F32),
        pltpu.VMEM((parts, rows, columns), F32),
        pltpu.VMEM((groups, 8, routes.size), F32),
        pltpu.VMEM((groups, parts, rows, width), BF16),
        pltpu.VMEM((owned, parts, per, deep), BF16),
        pltpu.VMEM((owned, groups, capacity, columns), BF16),
        pltpu.VMEM((groups, owned, capacity, columns), BF16),
        pltpu.VMEM((seqs, owned * per), F32),
        pltpu.SemaphoreType.DMA((3 * owned,)),
    ]
    scratch += dma(parts - 1) + dma(groups - 1) + dma(parts - 1) + dma(groups - 1)
    scratch += dma(groups) * 3 + dma(owned) * 3 + dma(owned * (groups - 1))
    return pl.pallas_call(
        functools.partial(experts_kernel, groups, parts, capacity),
        out_shape=jax.ShapeDtypeStruct((seqs, columns), BF16),
        in_specs=[vm] * 5 + [anyspace] * 3,
        out_specs=vm,
        scratch_shapes=scratch,
        compiler_params=pltpu.CompilerParams(
            collective_id=0, has_side_effects=True, vmem_limit_bytes=VMEM_BYTES
        ),
        name="experts",
    )(part, tokens, ffn_gain.reshape(1, -1), routes.T, logits.T, gate_w, up_w, down_w)


def slot_tables(routes, weights, expert_ids, capacity):
    blocks, seqs, top = routes.shape
    flat = routes.reshape(blocks, seqs * top)
    order = jnp.arange(seqs * top, dtype=jnp.int32)
    same = (flat[:, None, :] == flat[:, :, None]) & (order[None, None, :] < order[None, :, None])
    rank = jnp.sum(same.astype(jnp.int32), axis=2)
    match = flat[:, :, None] == expert_ids[None, None, :]
    hit = rank[:, :, None] == jnp.arange(capacity, dtype=jnp.int32)[None, None, :]
    table = (match[:, :, :, None] & hit[:, :, None, :]).astype(jnp.float32)
    table = table.reshape(blocks, seqs, top, expert_ids.shape[0], capacity)
    dispatch = jnp.sum(table, axis=2)
    combine = jnp.sum(table * weights[:, :, :, None, None], axis=2)
    return (dispatch, combine)


def run_experts(buffer, gate_w, up_w, down_w):
    gate = jnp.einsum("bjcd,jdf->bjcf", buffer, gate_w, preferred_element_type=jnp.float32)
    up = jnp.einsum("bjcd,jdf->bjcf", buffer, up_w, preferred_element_type=jnp.float32)
    bound_gate = jnp.minimum(gate, LIMIT)
    bound_up = jnp.clip(up, -LIMIT, LIMIT)
    hidden = ((bound_up + 1.0) * bound_gate * jax.nn.sigmoid(ALPHA * bound_gate)).astype(
        jnp.bfloat16
    )
    total = jnp.einsum(
        "bjcf,jfd->bjcd",
        lax.all_gather(hidden, "tp", axis=3, tiled=True),
        down_w,
        preferred_element_type=jnp.float32,
    )
    return total.astype(jnp.bfloat16)


def per_device(
    tokens,
    lengths,
    cache_keys,
    cache_values,
    attn_gain,
    q_first_w,
    q_second_w,
    k_first_w,
    k_second_w,
    value_w,
    mix_lambda,
    head_gain,
    out_w,
    ffn_gain,
    routes,
    route_logits,
    gate_w,
    up_w,
    down_w,
):
    groups, parts = lax.axis_size("ep"), lax.axis_size("tp")
    owned = gate_w.shape[0]
    seqs, top = routes.shape
    capacity = max(2, 2 * seqs * top // (owned * groups))
    fused = parts == 4 and seqs % (8 * parts) == 0 and capacity % 8 == 0 and seqs * top % 128 == 0
    partial_value = attend(
        tokens,
        lengths,
        cache_keys,
        cache_values,
        attn_gain,
        q_first_w,
        q_second_w,
        k_first_w,
        k_second_w,
        value_w,
        mix_lambda,
        head_gain,
        out_w,
        BF16 if fused else F32,
        parts if fused else 1,
    )
    if fused:
        return experts(
            partial_value, tokens, ffn_gain, routes, route_logits, gate_w, up_w, down_w, groups, parts, capacity
        )
    partial_value = partial_value.reshape(tokens.shape)
    wide = tokens.astype(F32)
    columns = wide.shape[1] // lax.axis_size("tp")
    start = lax.axis_index("tp") * columns
    summed = lax.psum(partial_value, "tp")
    after = wide + summed
    full_in = rms_scale(after, ffn_gain).astype(jnp.bfloat16)
    kept = lax.dynamic_slice_in_dim(after, start, columns, 1)
    weights = jax.nn.softmax(route_logits, axis=-1)
    expert_ids = jnp.arange(owned * groups, dtype=jnp.int32)
    dispatch, combine = slot_tables(routes[None], weights[None], expert_ids, capacity)
    buffer = jnp.einsum(
        "bsjc,bsd->bjcd",
        dispatch.astype(jnp.bfloat16),
        full_in[None],
        preferred_element_type=jnp.float32,
    ).astype(jnp.bfloat16)
    buffer = buffer.reshape(groups, owned, capacity, -1)
    arrived = lax.all_to_all(buffer, "ep", split_axis=0, concat_axis=0, tiled=True)
    results = run_experts(arrived, gate_w, up_w, down_w)
    returned = lax.all_to_all(results, "ep", split_axis=0, concat_axis=0, tiled=True).reshape(
        1, groups * owned, capacity, -1
    )
    moe = jnp.einsum(
        "bsjc,bjcd->bsd", combine, returned.astype(jnp.float32), precision=lax.Precision.HIGHEST
    )[0]
    return (kept + moe).astype(jnp.bfloat16)


def solution(mesh):
    return jax.shard_map(
        per_device,
        mesh=mesh,
        in_specs=(
            P("ep", None),
            P("ep"),
            P("ep", None, "tp"),
            P("ep", None, "tp"),
            P(),
            P(None, "tp"),
            P(None, "tp"),
            P(None, "tp"),
            P(None, "tp"),
            P(None, "tp"),
            P("tp"),
            P(),
            P("tp", None),
            P(),
            P("ep", None),
            P("ep", None),
            P("ep", None, "tp"),
            P("ep", None, "tp"),
            P("ep", None, "tp"),
        ),
        out_specs=P("ep", "tp"),
        check_vma=False,
    )
```

```python
import functools

import jax
import jax.numpy as jnp
from jax import lax
from jax.experimental import pallas as pl
from jax.experimental.pallas import tpu as pltpu
from jax.sharding import PartitionSpec as P

EPS = 1e-06
LIMIT = 7.0
ALPHA = 1.702
PIECE = 128
GROUP = 8
VMEM_BYTES = 67043328
LAYER_BYTES = 60 * 1024 * 1024
F32 = jnp.float32
BF16 = jnp.bfloat16


def attend_kernel(
    heads,
    lam_ref,
    lengths_hbm,
    tokens_hbm,
    again_hbm,
    hgain_hbm,
    keys_hbm,
    values_hbm,
    q1_hbm,
    q2_hbm,
    k1_hbm,
    k2_hbm,
    vw_hbm,
    ow_hbm,
    part_ref,
    kbuf,
    vbuf,
    q1_v,
    q2_v,
    k1_v,
    k2_v,
    vw_v,
    ow_v,
    queries,
    own_keys,
    new_values,
    attended,
    raw,
    weights_v,
    lengths_ref,
    tokens_ref,
    again_ref,
    hgain_ref,
    ksem,
    vsem,
    wsem,
    ssem,
):
    smalls = ((lengths_hbm, lengths_ref), (tokens_hbm, tokens_ref), (again_hbm, again_ref), (hgain_hbm, hgain_ref))
    smalls = [pltpu.make_async_copy(src, dst, ssem.at[i]) for i, (src, dst) in enumerate(smalls)]
    for small in smalls:
        small.start()
    seqs, length, width = kbuf.shape
    head = width // heads
    half = head // 2
    scale = half ** (-0.5)
    weights = ((q1_hbm, q1_v), (q2_hbm, q2_v), (k1_hbm, k1_v), (k2_hbm, k2_v), (vw_hbm, vw_v), (ow_hbm, ow_v))
    loads = [pltpu.make_async_copy(src, dst, wsem.at[i]) for i, (src, dst) in enumerate(weights)]
    for load in loads[:5]:
        load.start()

    def fetch(s):
        rows = pl.multiple_of((lengths_ref[s] + (PIECE - 1)) // PIECE * PIECE, PIECE)
        return (
            pltpu.make_async_copy(keys_hbm.at[s, pl.ds(0, rows)], kbuf.at[s, pl.ds(0, rows)], ksem.at[s]),
            pltpu.make_async_copy(values_hbm.at[s, pl.ds(0, rows)], vbuf.at[s, pl.ds(0, rows)], vsem.at[s]),
        )

    def start(s, carry):
        a, b = fetch(s)
        a.start()
        b.start()
        return carry

    smalls[0].wait()
    lax.fori_loop(0, seqs, start, 0)
    loads[5].start()
    for small in smalls[1:]:
        small.wait()

    wide = tokens_ref[...].astype(F32)
    normed = (
        wide * lax.rsqrt(jnp.mean(wide * wide, axis=-1, keepdims=True) + EPS) * again_ref[...]
    ).astype(BF16)
    for load in loads[:5]:
        load.wait()

    def project(w):
        return jnp.dot(normed, w[...], preferred_element_type=F32).astype(BF16).astype(F32)

    q1, q2, k1, k2 = project(q1_v), project(q2_v), project(k1_v), project(k2_v)
    new_values[...] = project(vw_v)
    zero = jnp.zeros((seqs, half), F32)
    queries[...] = jnp.zeros_like(queries)
    kparts = []
    for h in range(heads):
        cut = slice(h * half, (h + 1) * half)
        kparts += [k1[:, cut], k2[:, cut]]
        for p, q in ((0, q1), (1, q2)):
            parts = [zero] * (2 * heads)
            parts[2 * h + p] = q[:, cut]
            queries[:, 4 * p + h, :] = jnp.concatenate(parts, axis=-1)
    own_keys[...] = jnp.concatenate(kparts, axis=-1)

    position = lax.broadcasted_iota(jnp.int32, (8, length), 1)
    row = lax.broadcasted_iota(jnp.int32, (8, width), 0)
    mine = row == lax.broadcasted_iota(jnp.int32, (8, width), 1) // head
    map_row = lax.broadcasted_iota(jnp.int32, (8, 1), 0)
    lam = jnp.zeros((8, 1), F32)
    for h in range(heads):
        lam = jnp.where(map_row == h, lam_ref[h], lam)
    hgain = jnp.concatenate([hgain_ref[...]] * heads, axis=-1)

    def group_step(g, carry):
        for j in range(GROUP):
            for copy in fetch(g * GROUP + j):
                copy.wait()
        for j in range(GROUP):
            s = g * GROUP + j
            raw[j] = lax.dot_general(
                queries[s].astype(BF16), kbuf[s], (((1,), (1,)), ((), ())), preferred_element_type=F32
            )
        own_ws = []
        for j in range(GROUP):
            s = g * GROUP + j
            own = jnp.sum(queries[s] * own_keys[pl.ds(s, 1), :], axis=-1, keepdims=True) * scale
            scores = jnp.where(position < lengths_ref[s], raw[j] * scale, -jnp.inf)
            top = jnp.maximum(jnp.max(scores, axis=-1, keepdims=True), own)
            raised = jnp.exp(scores - top)
            own_raised = jnp.exp(own - top)
            total = jnp.sum(raised, axis=-1, keepdims=True) + own_raised
            inv = 1.0 / total
            probs = raised * inv
            own_probs = own_raised * inv
            weights_v[j] = (probs - lam * pltpu.roll(probs, 4, 0)).astype(BF16)
            own_b = jnp.broadcast_to(own_probs, (8, 128))
            own_ws.append((own_b - lam * pltpu.roll(own_b, 4, 0)).astype(BF16).astype(F32)[:, :1])
        outs = []
        for j in range(GROUP):
            s = g * GROUP + j
            count = lengths_ref[s]
            pieces = [
                jnp.where(c * PIECE < count, vbuf[s, c * PIECE:(c + 1) * PIECE, :], jnp.zeros((PIECE, width), BF16))
                for c in range(length // PIECE)
            ]
            outs.append(jnp.dot(weights_v[j], jnp.concatenate(pieces, axis=0), preferred_element_type=F32))
        for j in range(GROUP):
            s = g * GROUP + j
            out = outs[j] + own_ws[j] * new_values[pl.ds(s, 1), :]
            out = jnp.where(mine, out, 0.0)
            mean_sq = jnp.sum(out * out, axis=-1, keepdims=True) * (1.0 / head)
            out = out * lax.rsqrt(mean_sq + EPS)
            attended[pl.ds(s, 1), :] = jnp.sum(out, axis=0, keepdims=True) * hgain
        return carry

    lax.fori_loop(0, seqs // GROUP, group_step, 0)
    loads[5].wait()
    part_ref[...] = jnp.dot(
        attended[...].astype(BF16), ow_v[...], preferred_element_type=F32
    ).reshape(part_ref.shape).astype(part_ref.dtype)


def attend(
    tokens, lengths, cache_keys, cache_values, attn_gain, q1w, q2w, k1w, k2w, vw, lam, hgain, out_w, out_dtype, parts
):
    seqs, length, width = cache_keys.shape
    heads = lam.shape[0]
    vm = pl.BlockSpec(memory_space=pltpu.VMEM)
    anyspace = pl.BlockSpec(memory_space=pltpu.HBM)
    scratch = [pltpu.VMEM(cache_keys.shape, BF16), pltpu.VMEM(cache_values.shape, BF16)]
    scratch += [pltpu.VMEM(w.shape, BF16) for w in (q1w, q2w, k1w, k2w, vw, out_w)]
    scratch += [
        pltpu.VMEM((seqs, 8, width), F32),
        pltpu.VMEM((seqs, width), F32),
        pltpu.VMEM((seqs, width), F32),
        pltpu.VMEM((seqs, width), F32),
        pltpu.VMEM((GROUP, 8, length), F32),
        pltpu.VMEM((GROUP, 8, length), BF16),
        pltpu.SMEM((seqs,), jnp.int32),
        pltpu.VMEM(tokens.shape, BF16),
        pltpu.VMEM((1, tokens.shape[1]), F32),
        pltpu.VMEM((1, hgain.shape[0]), F32),
        pltpu.SemaphoreType.DMA((seqs,)),
        pltpu.SemaphoreType.DMA((seqs,)),
        pltpu.SemaphoreType.DMA((6,)),
        pltpu.SemaphoreType.DMA((4,)),
    ]
    return pl.pallas_call(
        functools.partial(attend_kernel, heads),
        out_shape=jax.ShapeDtypeStruct((parts, seqs // parts, out_w.shape[1]), out_dtype),
        in_specs=[pl.BlockSpec(memory_space=pltpu.SMEM)] + [anyspace] * 12,
        out_specs=vm,
        scratch_shapes=scratch,
        compiler_params=pltpu.CompilerParams(vmem_limit_bytes=VMEM_BYTES),
        name="attend",
    )(
        lam, lengths, tokens, attn_gain.reshape(1, -1), hgain.reshape(1, -1),
        cache_keys, cache_values, q1w, q2w, k1w, k2w, vw, out_w,
    )


MESH = pl.DeviceIdType.MESH


def rms_scale(rows, gain):
    mean_sq = jnp.mean(rows * rows, axis=-1, keepdims=True)
    return rows * lax.rsqrt(mean_sq + EPS) * gain


def exact_dot(a, b):
    return jnp.dot(a, b, precision=lax.Precision.HIGHEST, preferred_element_type=F32)


def where_is(shape, dim):
    return lax.broadcasted_iota(jnp.int32, shape, dim)


def turned_dot(a, b, left, right):
    return lax.dot_general(
        a, b, (((left,), (right,)), ((), ())), precision=lax.Precision.HIGHEST, preferred_element_type=F32
    )


def route_tables(routes, logits, slots, capacity):
    top, seqs = routes.shape
    n = seqs * top
    routes = routes.astype(F32)
    spread = turned_dot(routes, (where_is((top, n), 1) % top == where_is((top, n), 0)).astype(F32), 0, 0)
    row = jnp.sum(jnp.where(where_is((seqs, n), 1) // top == where_is((seqs, n), 0), spread, 0.0), axis=0, keepdims=True)
    owner = (where_is((n, seqs), 0) // top == where_is((n, seqs), 1)).astype(F32)
    pick = where_is((n, top), 0) % top == where_is((n, top), 1)
    col = jnp.sum(jnp.where(pick, turned_dot(owner, routes, 1, 1), 0.0), axis=1, keepdims=True)
    same = row == col
    i, j = where_is((n, n), 0), where_is((n, n), 1)
    rank_col = jnp.sum((same & (j < i)).astype(F32), axis=1, keepdims=True)
    rank_row = jnp.sum((same & (i < j)).astype(F32), axis=0, keepdims=True)
    slot_row = row * capacity + rank_row
    return slot_row, lambda: combine_table(logits, col, rank_col, owner, pick, slots, capacity)


def combine_table(logits, col, rank_col, owner, pick, slots, capacity):
    n, seqs = owner.shape
    top = n // seqs
    slot_col = col * capacity + rank_col
    raised = jnp.exp(logits - jnp.max(logits, axis=0, keepdims=True))
    weights = raised / jnp.sum(raised, axis=0, keepdims=True)
    weight_col = jnp.sum(jnp.where(pick, turned_dot(owner, weights, 1, 1), 0.0), axis=1, keepdims=True)
    hit = where_is((n, slots), 1).astype(F32) == slot_col
    member = (where_is((seqs, n), 1) // top == where_is((seqs, n), 0)).astype(F32)
    combine = exact_dot(member, jnp.where(hit, weight_col, 0.0))
    return combine


def flip(index, mask):
    bit = 1
    out = index
    while bit <= mask:
        if mask & bit:
            out = out + (1 - 2 * lax.rem(index // bit, 2)) * bit
        bit *= 2
    return out


def layer_kernel(
    heads,
    groups,
    parts,
    capacity,
    lam_hbm,
    lengths_hbm,
    tokens_hbm,
    again_hbm,
    hgain_hbm,
    fgain_hbm,
    routes_hbm,
    logits_hbm,
    keys_hbm,
    values_hbm,
    q1_hbm,
    q2_hbm,
    k1_hbm,
    k2_hbm,
    vw_hbm,
    ow_hbm,
    gate_hbm,
    up_hbm,
    down_hbm,
    out_ref,
    kbuf,
    vbuf,
    q1_v,
    q2_v,
    k1_v,
    k2_v,
    vw_v,
    ow_v,
    gate_v,
    up_v,
    down_v,
    queries,
    own_keys,
    new_values,
    attended,
    raw,
    weights_v,
    lam_ref,
    lengths_ref,
    tokens_ref,
    again_ref,
    hgain_ref,
    fgain_ref,
    routes_ref,
    logits_ref,
    wide_v,
    part_f,
    part_b,
    rs_buf,
    kept,
    slot_buf,
    combine_v,
    xbuf,
    hbuf,
    resbuf,
    ret,
    ksem,
    vsem,
    wsem,
    ssem,
    snd,
    rs_r,
    sl_r,
    ag_r,
    far_r,
    near_r,
    relay_r,
    tail_r,
    hy_r,
    hc_r,
    hd_r,
    re_r,
):
    e, t = lax.axis_index("ep"), lax.axis_index("tp")
    seqs, length, width = kbuf.shape
    head = width // heads
    half = head // 2
    scale = half ** (-0.5)
    owned = gate_v.shape[0]
    columns = out_ref.shape[1]
    pieces = seqs // GROUP
    top = routes_ref.shape[0]
    n = seqs * top
    block = owned * capacity
    per = groups * capacity
    twin = t + 1 - 2 * lax.rem(t, 2)
    across = lax.rem(t + 2, parts)

    smalls = (
        (lengths_hbm, lengths_ref), (tokens_hbm, tokens_ref), (again_hbm, again_ref), (hgain_hbm, hgain_ref),
        (fgain_hbm, fgain_ref), (routes_hbm, routes_ref), (logits_hbm, logits_ref), (lam_hbm, lam_ref),
    )
    smalls = [pltpu.make_async_copy(src, dst, ssem.at[i]) for i, (src, dst) in enumerate(smalls)]
    for small in smalls:
        small.start()
    weights = [(q1_hbm, q1_v), (q2_hbm, q2_v), (k1_hbm, k1_v), (k2_hbm, k2_v), (vw_hbm, vw_v), (ow_hbm, ow_v)]
    for j in range(owned):
        for src, dst in ((gate_hbm, gate_v), (up_hbm, up_v), (down_hbm, down_v)):
            weights.append((src.at[j], dst.at[j]))
    loads = [pltpu.make_async_copy(src, dst, wsem.at[i]) for i, (src, dst) in enumerate(weights)]
    for load in loads[:5]:
        load.start()

    def arrived(ref, sem):
        pltpu.make_async_copy(ref, ref, sem).wait()

    def fetch_keys(s):
        return pltpu.make_async_copy(keys_hbm.at[s], kbuf.at[s], ksem.at[s // GROUP])

    def fetch_values(s):
        return pltpu.make_async_copy(values_hbm.at[s], vbuf.at[s], vsem.at[s // GROUP])

    def start_all(fetch, g):
        if g < pieces:
            for j in range(GROUP):
                fetch(g * GROUP + j).start()

    start_all(fetch_keys, 0)

    barrier = pltpu.get_barrier_semaphore()
    for k in range(1, parts):
        pl.semaphore_signal(barrier, inc=1, device_id=(e, lax.rem(t + k, parts)), device_id_type=MESH)
    for m in range(1, groups):
        pl.semaphore_signal(barrier, inc=1, device_id=(flip(e, m), t), device_id_type=MESH)

    def remote(src, dst, s_sem, r_sem, device):
        return pltpu.make_async_remote_copy(
            src_ref=src, dst_ref=dst, send_sem=s_sem, recv_sem=r_sem, device_id=device, device_id_type=MESH
        )

    def send(src, dst, s_sem, r_sem, device):
        copy = remote(src, dst, snd.at[s_sem], r_sem, device)
        copy.start()
        return copy

    for i in (1, 2):
        smalls[i].wait()
    start_all(fetch_values, 0)
    loads[5].start()
    start_all(fetch_keys, 1)
    wide = tokens_ref[...].astype(F32)
    wide_v[...] = wide
    own_columns = pl.ds(pl.multiple_of(t * columns, columns), columns)
    kept[...] = wide_v[:, own_columns].reshape(kept.shape)
    normed = (
        wide * lax.rsqrt(jnp.mean(wide * wide, axis=-1, keepdims=True) + EPS) * again_ref[...]
    ).astype(BF16)
    for load in loads[:5]:
        load.wait()

    def project(w):
        return jnp.dot(normed, w[...], preferred_element_type=F32).astype(BF16).astype(F32)

    q1, q2, k1, k2 = project(q1_v), project(q2_v), project(k1_v), project(k2_v)
    new_values[...] = project(vw_v)
    zero = jnp.zeros((seqs, half), F32)
    queries[...] = jnp.zeros_like(queries)
    kparts = []
    for h in range(heads):
        cut = slice(h * half, (h + 1) * half)
        kparts += [k1[:, cut], k2[:, cut]]
        for p, q in ((0, q1), (1, q2)):
            mixed = [zero] * (2 * heads)
            mixed[2 * h + p] = q[:, cut]
            queries[:, 4 * p + h, :] = jnp.concatenate(mixed, axis=-1)
    own_keys[...] = jnp.concatenate(kparts, axis=-1)

    for i in (0, 3, 4, 5, 6, 7):
        smalls[i].wait()
    fgain = fgain_ref[:, own_columns]
    position = lax.broadcasted_iota(jnp.int32, (8, length), 1)
    row = lax.broadcasted_iota(jnp.int32, (8, width), 0)
    mine = row == lax.broadcasted_iota(jnp.int32, (8, width), 1) // head
    map_row = lax.broadcasted_iota(jnp.int32, (8, 1), 0)
    lam = jnp.zeros((8, 1), F32)
    for h in range(heads):
        lam = jnp.where(map_row == h, lam_ref[h], lam)
    hgain = jnp.concatenate([hgain_ref[...]] * heads, axis=-1)
    lane = lax.broadcasted_iota(jnp.int32, (GROUP, 128), 1)

    def attention(g):
        arrived(kbuf.at[pl.ds(g * GROUP, GROUP)], ksem.at[g])
        start_all(fetch_values, g + 1)
        for j in range(GROUP):
            s = g * GROUP + j
            raw[j] = lax.dot_general(
                queries[s].astype(BF16), kbuf[s], (((1,), (1,)), ((), ())), preferred_element_type=F32
            )
        own_ws = []
        for j in range(GROUP):
            s = g * GROUP + j
            own = jnp.sum(queries[s] * own_keys[pl.ds(s, 1), :], axis=-1, keepdims=True) * scale
            scores = jnp.where(position < lengths_ref[s], raw[j] * scale, -jnp.inf)
            highest = jnp.maximum(jnp.max(scores, axis=-1, keepdims=True), own)
            raised = jnp.exp(scores - highest)
            own_raised = jnp.exp(own - highest)
            total = jnp.sum(raised, axis=-1, keepdims=True) + own_raised
            inv = 1.0 / total
            probs = raised * inv
            own_probs = own_raised * inv
            weights_v[j] = (probs - lam * pltpu.roll(probs, 4, 0)).astype(BF16)
            own_b = jnp.broadcast_to(own_probs, (8, 128))
            own_ws.append((own_b - lam * pltpu.roll(own_b, 4, 0)).astype(BF16).astype(F32)[:, :1])
        arrived(vbuf.at[pl.ds(g * GROUP, GROUP)], vsem.at[g])
        start_all(fetch_keys, g + 2)
        outs = [
            jnp.dot(weights_v[j], vbuf[g * GROUP + j], preferred_element_type=F32) for j in range(GROUP)
        ]
        for j in range(GROUP):
            s = g * GROUP + j
            out = outs[j] + own_ws[j] * new_values[pl.ds(s, 1), :]
            out = jnp.where(mine, out, 0.0)
            mean_sq = jnp.sum(out * out, axis=-1, keepdims=True) * (1.0 / head)
            out = out * lax.rsqrt(mean_sq + EPS)
            attended[pl.ds(s, 1), :] = jnp.sum(out, axis=0, keepdims=True) * hgain

    def send_partials(g):
        heads_out = attended[g * GROUP:(g + 1) * GROUP, :].astype(BF16)
        partial = jnp.dot(heads_out, ow_v[...], preferred_element_type=F32)
        for q in range(parts):
            cut = partial[:, q * columns:(q + 1) * columns]
            part_f[q] = cut
            part_b[g, q] = cut.astype(BF16)
        for k in range(1, parts):
            peer = lax.rem(t + k, parts)
            send(part_b.at[g, peer], rs_buf.at[g, k - 1], 0, rs_r.at[g], (e, peer))
        kept[g] = kept[g] + part_f[t]

    gather, far, tail = {}, {}, {}
    opposite = lax.rem(twin + 2, parts)
    last = pieces - 1

    def late(g, m):
        return g == last and m >= groups // 2

    def forward(g, m):
        view = xbuf.at[g, t, flip(e, m)]
        far[g, m] = send(view, view, 3, far_r.at[g, m], (e, across))
        if late(g, m):
            tail[m] = send(view, view, 3, tail_r.at[m], (e, opposite))
        send(view, view, 3, near_r.at[0], (e, twin))

    def relay_rows(g):
        for m in range(groups):
            far[g, m].wait_recv()
            if not late(g, m):
                view = xbuf.at[g, across, flip(e, m)]
                send(view, view, 3, relay_r.at[int(g == last)], (e, twin))

    def send_rows(g):
        arrived(rs_buf.at[g], rs_r.at[g])
        total = kept[g]
        for k in range(1, parts):
            total = total + rs_buf[g, k - 1].astype(F32)
        kept[g] = total
        squares = jnp.sum(total * total, axis=-1, keepdims=True)
        high = jnp.broadcast_to(squares, (GROUP, 128)).astype(BF16)
        low = jnp.broadcast_to(squares, (GROUP, 128)) - high.astype(F32)
        xbuf[g, t, e, :, :columns] = (total * fgain).astype(BF16)
        xbuf[g, t, e, :, columns:] = jnp.where(lane < 64, high.astype(F32), low).astype(BF16)
        view = xbuf.at[g, t, e]
        for m in range(groups - 1, 0, -1):
            gather[g, m] = send(view, view, 2, ag_r.at[g, m - 1], (flip(e, m), t))
        forward(g, 0)

    def forward_rows(g):
        for m in range(1, groups):
            gather[g, m].wait_recv()
            forward(g, m)

    for g in range(pieces):
        attention(g)
        if g == 0:
            pl.semaphore_wait(barrier, parts + groups - 2)
            loads[5].wait()
        send_partials(g)
        if g >= 1:
            send_rows(g - 1)
        if g >= 2:
            forward_rows(g - 2)
        if g >= 3:
            relay_rows(g - 3)

    fetches = loads[6:]
    third = owned
    for load in fetches[:third]:
        load.start()
    slot_row, later = route_tables(routes_ref[...], logits_ref[...], groups * block, capacity)
    slot_buf[e] = jnp.broadcast_to(slot_row, (8, n))
    for m in range(groups - 1, 0, -1):
        send(slot_buf.at[e], slot_buf.at[e], 1, sl_r.at[0], (flip(e, m), t))
    combine_v[...] = later()
    send_rows(last)
    for load in fetches[third:]:
        load.start()
    for g in range(max(pieces - 3, 0), pieces - 2):
        relay_rows(g)
    forward_rows(pieces - 2)
    forward_rows(last)
    arrived(slot_buf.at[pl.ds(0, groups - 1)], sl_r.at[0])
    base = e * block
    local = (where_is((block, n), 0) + base).astype(F32)
    tokens_all = groups * seqs
    token = where_is((n, tokens_all), 0) // top
    spot_row = token // GROUP * (groups * GROUP) + token % GROUP
    place = []
    for b in range(groups):
        chosen = (slot_buf[b][:1, :] == local).astype(BF16)
        spot = (where_is((n, tokens_all), 1) == spot_row + b * GROUP).astype(BF16)
        placed = jnp.dot(chosen, spot, preferred_element_type=F32)
        place.append(placed.reshape(owned, 1, capacity, tokens_all))
    dispatch = jnp.concatenate(place, axis=1).reshape(groups * block, tokens_all).astype(BF16)

    relay_rows(pieces - 2)
    relay_rows(last)
    arrived(xbuf.at[:, 0], near_r.at[0])
    arrived(xbuf.at[pl.ds(0, last), 0], relay_r.at[0])
    arrived(xbuf.at[last, 0, pl.ds(0, groups // 2)], relay_r.at[1])
    for copy in tail.values():
        copy.wait_recv()

    lines, squares = [], jnp.zeros((groups * block, 128), F32)
    for q in range(parts):
        rows = xbuf[:, q].astype(F32).reshape(tokens_all, columns + 128).astype(BF16)
        picked = jnp.dot(dispatch, rows, preferred_element_type=F32)
        lines.append(picked[:, :columns].astype(BF16))
        squares = squares + picked[:, columns:]
    lines = jnp.concatenate(lines, axis=-1)
    mean_sq = (squares[:, :1] + squares[:, 64:65]) * (1.0 / (columns * parts))
    row_scale = lax.rsqrt(mean_sq + EPS)
    hfar, hnear = [], []
    for j in range(owned):
        for i in range(2):
            loads[6 + 3 * j + i].wait()
        line = lines[j * per:(j + 1) * per]
        line_scale = row_scale[j * per:(j + 1) * per]
        gate = jnp.minimum(jnp.dot(line, gate_v[j], preferred_element_type=F32) * line_scale, LIMIT)
        up = jnp.clip(jnp.dot(line, up_v[j], preferred_element_type=F32) * line_scale, -LIMIT, LIMIT)
        hbuf[j, t] = ((up + 1.0) * gate * jax.nn.sigmoid(ALPHA * gate)).astype(BF16)
        view = hbuf.at[j, t]
        hfar.append(send(view, view, 4, hy_r.at[j], (e, across)))
        if j == 0:
            hrelay = [send(view, view, 4, hd_r.at[j], (e, opposite))]
        hnear.append(send(view, view, 4, hc_r.at[j], (e, twin)))
    deep = hbuf.shape[3]
    for j in range(owned + 1):
        if j < owned:
            hfar[j].wait_recv()
            theirs = hbuf.at[j, across]
            if j:
                hrelay.append(send(theirs, theirs, 4, hd_r.at[j], (e, twin)))
        if j == 0:
            continue
        i = j - 1
        hnear[i].wait_recv()
        hrelay[i].wait_recv()
        loads[6 + 3 * i + 2].wait()
        result = jnp.zeros((per, columns), F32)
        for q in range(parts):
            result += jnp.dot(hbuf[i, q], down_v[i, q * deep:(q + 1) * deep, :], preferred_element_type=F32)
        resbuf[i] = result.reshape(groups, capacity, columns).astype(BF16)
        for m in range(groups - 1, 0, -1):
            peer = flip(e, m)
            send(resbuf.at[i, peer], ret.at[e, i], 5, re_r.at[0], (peer, t))
        ret[e, i] = resbuf[i, e]
    arrived(ret.at[pl.ds(0, groups - 1)], re_r.at[0])
    moe = exact_dot(combine_v[...], ret[...].astype(F32).reshape(groups * block, columns))
    out_ref[...] = (kept[...].reshape(seqs, columns) + moe).astype(out_ref.dtype)
    arrived(part_b.at[:, pl.ds(0, parts - 1)], snd.at[0])
    arrived(slot_buf.at[pl.ds(0, groups - 1)], snd.at[1])
    arrived(xbuf.at[:, 0, pl.ds(0, groups - 1)], snd.at[2])
    arrived(xbuf.at[:, pl.ds(0, parts - 1)], snd.at[3])
    arrived(hbuf.at[:, pl.ds(0, parts - 1)], snd.at[4])
    arrived(resbuf.at[:, pl.ds(0, groups - 1)], snd.at[5])


def layer(
    tokens, lengths, cache_keys, cache_values, attn_gain, q1w, q2w, k1w, k2w, vw, lam, hgain, out_w,
    ffn_gain, routes, logits, gate_w, up_w, down_w, groups, parts, capacity,
):
    seqs, length, width = cache_keys.shape
    heads = lam.shape[0]
    owned, _, deep = gate_w.shape
    columns = down_w.shape[2]
    per = groups * capacity
    pieces = seqs // GROUP
    full = tokens.shape[1]
    routes, logits = routes.T, logits.T
    anyspace = pl.BlockSpec(memory_space=pltpu.HBM)
    scratch = [pltpu.VMEM(cache_keys.shape, BF16), pltpu.VMEM(cache_values.shape, BF16)]
    scratch += [pltpu.VMEM(w.shape, BF16) for w in (q1w, q2w, k1w, k2w, vw, out_w, gate_w, up_w, down_w)]
    scratch += [
        pltpu.VMEM((seqs, 8, width), F32),
        pltpu.VMEM((seqs, width), F32),
        pltpu.VMEM((seqs, width), F32),
        pltpu.VMEM((seqs, width), F32),
        pltpu.VMEM((GROUP, 8, length), F32),
        pltpu.VMEM((GROUP, 8, length), BF16),
        pltpu.SMEM(lam.shape, F32),
        pltpu.SMEM((seqs,), jnp.int32),
        pltpu.VMEM(tokens.shape, BF16),
        pltpu.VMEM((1, full), F32),
        pltpu.VMEM((1, hgain.shape[0]), F32),
        pltpu.VMEM((1, full), F32),
        pltpu.VMEM(routes.shape, routes.dtype),
        pltpu.VMEM(logits.shape, F32),
        pltpu.VMEM(tokens.shape, F32),
        pltpu.VMEM((parts, GROUP, columns), F32),
        pltpu.VMEM((pieces, parts, GROUP, columns), BF16),
        pltpu.VMEM((pieces, parts - 1, GROUP, columns), BF16),
        pltpu.VMEM((pieces, GROUP, columns), F32),
        pltpu.VMEM((groups, 8, routes.size), F32),
        pltpu.VMEM((seqs, owned * per), F32),
        pltpu.VMEM((pieces, parts, groups, GROUP, columns + 128), BF16),
        pltpu.VMEM((owned, parts, per, deep), BF16),
        pltpu.VMEM((owned, groups, capacity, columns), BF16),
        pltpu.VMEM((groups, owned, capacity, columns), BF16),
    ]
    dma = lambda *shape: [pltpu.SemaphoreType.DMA(shape)]
    scratch += dma(pieces) * 2 + dma(6 + 3 * owned) + dma(8)
    scratch += dma(6) + dma(pieces) + dma(1) + dma(pieces, groups - 1)
    scratch += dma(pieces, groups) + dma(1) + dma(2) + dma(groups) + dma(owned) * 3 + dma(1)
    return pl.pallas_call(
        functools.partial(layer_kernel, heads, groups, parts, capacity),
        out_shape=jax.ShapeDtypeStruct((seqs, columns), BF16),
        in_specs=[anyspace] * 19,
        out_specs=pl.BlockSpec(memory_space=pltpu.VMEM),
        scratch_shapes=scratch,
        compiler_params=pltpu.CompilerParams(
            collective_id=0, has_side_effects=True, vmem_limit_bytes=LAYER_BYTES
        ),
        name="layer",
    )(
        lam, lengths, tokens, attn_gain.reshape(1, -1), hgain.reshape(1, -1), ffn_gain.reshape(1, -1),
        routes, logits, cache_keys, cache_values, q1w, q2w, k1w, k2w, vw, out_w, gate_w, up_w, down_w,
    )


def slot_tables(routes, weights, expert_ids, capacity):
    blocks, seqs, top = routes.shape
    flat = routes.reshape(blocks, seqs * top)
    order = jnp.arange(seqs * top, dtype=jnp.int32)
    same = (flat[:, None, :] == flat[:, :, None]) & (order[None, None, :] < order[None, :, None])
    rank = jnp.sum(same.astype(jnp.int32), axis=2)
    match = flat[:, :, None] == expert_ids[None, None, :]
    hit = rank[:, :, None] == jnp.arange(capacity, dtype=jnp.int32)[None, None, :]
    table = (match[:, :, :, None] & hit[:, :, None, :]).astype(jnp.float32)
    table = table.reshape(blocks, seqs, top, expert_ids.shape[0], capacity)
    dispatch = jnp.sum(table, axis=2)
    combine = jnp.sum(table * weights[:, :, :, None, None], axis=2)
    return (dispatch, combine)


def run_experts(buffer, gate_w, up_w, down_w):
    gate = jnp.einsum("bjcd,jdf->bjcf", buffer, gate_w, preferred_element_type=jnp.float32)
    up = jnp.einsum("bjcd,jdf->bjcf", buffer, up_w, preferred_element_type=jnp.float32)
    bound_gate = jnp.minimum(gate, LIMIT)
    bound_up = jnp.clip(up, -LIMIT, LIMIT)
    hidden = ((bound_up + 1.0) * bound_gate * jax.nn.sigmoid(ALPHA * bound_gate)).astype(
        jnp.bfloat16
    )
    total = jnp.einsum(
        "bjcf,jfd->bjcd",
        lax.all_gather(hidden, "tp", axis=3, tiled=True),
        down_w,
        preferred_element_type=jnp.float32,
    )
    return total.astype(jnp.bfloat16)


def per_device(
    tokens,
    lengths,
    cache_keys,
    cache_values,
    attn_gain,
    q_first_w,
    q_second_w,
    k_first_w,
    k_second_w,
    value_w,
    mix_lambda,
    head_gain,
    out_w,
    ffn_gain,
    routes,
    route_logits,
    gate_w,
    up_w,
    down_w,
):
    groups, parts = lax.axis_size("ep"), lax.axis_size("tp")
    owned = gate_w.shape[0]
    seqs, top = routes.shape
    capacity = max(2, 2 * seqs * top // (owned * groups))
    fused = (
        parts == 4 and seqs % GROUP == 0 and capacity % 8 == 0 and seqs * top % 128 == 0 and groups & (groups - 1) == 0
    )
    if fused:
        return layer(
            tokens, lengths, cache_keys, cache_values, attn_gain, q_first_w, q_second_w, k_first_w, k_second_w,
            value_w, mix_lambda, head_gain, out_w, ffn_gain, routes, route_logits, gate_w, up_w, down_w,
            groups, parts, capacity,
        )
    partial_value = attend(
        tokens,
        lengths,
        cache_keys,
        cache_values,
        attn_gain,
        q_first_w,
        q_second_w,
        k_first_w,
        k_second_w,
        value_w,
        mix_lambda,
        head_gain,
        out_w,
        F32,
        1,
    )
    partial_value = partial_value.reshape(tokens.shape)
    wide = tokens.astype(F32)
    columns = wide.shape[1] // lax.axis_size("tp")
    start = lax.axis_index("tp") * columns
    summed = lax.psum(partial_value, "tp")
    after = wide + summed
    full_in = rms_scale(after, ffn_gain).astype(jnp.bfloat16)
    kept = lax.dynamic_slice_in_dim(after, start, columns, 1)
    weights = jax.nn.softmax(route_logits, axis=-1)
    expert_ids = jnp.arange(owned * groups, dtype=jnp.int32)
    dispatch, combine = slot_tables(routes[None], weights[None], expert_ids, capacity)
    buffer = jnp.einsum(
        "bsjc,bsd->bjcd",
        dispatch.astype(jnp.bfloat16),
        full_in[None],
        preferred_element_type=jnp.float32,
    ).astype(jnp.bfloat16)
    buffer = buffer.reshape(groups, owned, capacity, -1)
    arrived = lax.all_to_all(buffer, "ep", split_axis=0, concat_axis=0, tiled=True)
    results = run_experts(arrived, gate_w, up_w, down_w)
    returned = lax.all_to_all(results, "ep", split_axis=0, concat_axis=0, tiled=True).reshape(
        1, groups * owned, capacity, -1
    )
    moe = jnp.einsum(
        "bsjc,bjcd->bsd", combine, returned.astype(jnp.float32), precision=lax.Precision.HIGHEST
    )[0]
    return (kept + moe).astype(jnp.bfloat16)


def solution(mesh):
    return jax.shard_map(
        per_device,
        mesh=mesh,
        in_specs=(
            P("ep", None),
            P("ep"),
            P("ep", None, "tp"),
            P("ep", None, "tp"),
            P(),
            P(None, "tp"),
            P(None, "tp"),
            P(None, "tp"),
            P(None, "tp"),
            P(None, "tp"),
            P("tp"),
            P(),
            P("tp", None),
            P(),
            P("ep", None),
            P("ep", None),
            P("ep", None, "tp"),
            P("ep", None, "tp"),
            P("ep", None, "tp"),
        ),
        out_specs=P("ep", "tp"),
        check_vma=False,
    )
```

```python
import functools

import jax
import jax.numpy as jnp
from jax import lax
from jax.experimental import pallas as pl
from jax.experimental.pallas import tpu as pltpu
from jax.sharding import PartitionSpec as P

EPS = 1e-06
LIMIT = 7.0
ALPHA = 1.702
PIECE = 128
GROUP = 8
VMEM_BYTES = 67043328
LAYER_BYTES = 60 * 1024 * 1024
F32 = jnp.float32
BF16 = jnp.bfloat16


def attend_kernel(
    heads,
    lam_ref,
    lengths_hbm,
    tokens_hbm,
    again_hbm,
    hgain_hbm,
    keys_hbm,
    values_hbm,
    q1_hbm,
    q2_hbm,
    k1_hbm,
    k2_hbm,
    vw_hbm,
    ow_hbm,
    part_ref,
    kbuf,
    vbuf,
    q1_v,
    q2_v,
    k1_v,
    k2_v,
    vw_v,
    ow_v,
    queries,
    own_keys,
    new_values,
    attended,
    raw,
    weights_v,
    lengths_ref,
    tokens_ref,
    again_ref,
    hgain_ref,
    ksem,
    vsem,
    wsem,
    ssem,
):
    smalls = ((lengths_hbm, lengths_ref), (tokens_hbm, tokens_ref), (again_hbm, again_ref), (hgain_hbm, hgain_ref))
    smalls = [pltpu.make_async_copy(src, dst, ssem.at[i]) for i, (src, dst) in enumerate(smalls)]
    for small in smalls:
        small.start()
    seqs, length, width = kbuf.shape
    head = width // heads
    half = head // 2
    scale = half ** (-0.5)
    weights = ((q1_hbm, q1_v), (q2_hbm, q2_v), (k1_hbm, k1_v), (k2_hbm, k2_v), (vw_hbm, vw_v), (ow_hbm, ow_v))
    loads = [pltpu.make_async_copy(src, dst, wsem.at[i]) for i, (src, dst) in enumerate(weights)]
    for load in loads[:5]:
        load.start()

    def fetch(s):
        rows = pl.multiple_of((lengths_ref[s] + (PIECE - 1)) // PIECE * PIECE, PIECE)
        return (
            pltpu.make_async_copy(keys_hbm.at[s, pl.ds(0, rows)], kbuf.at[s, pl.ds(0, rows)], ksem.at[s]),
            pltpu.make_async_copy(values_hbm.at[s, pl.ds(0, rows)], vbuf.at[s, pl.ds(0, rows)], vsem.at[s]),
        )

    def start(s, carry):
        a, b = fetch(s)
        a.start()
        b.start()
        return carry

    smalls[0].wait()
    lax.fori_loop(0, seqs, start, 0)
    loads[5].start()
    for small in smalls[1:]:
        small.wait()

    wide = tokens_ref[...].astype(F32)
    normed = (
        wide * lax.rsqrt(jnp.mean(wide * wide, axis=-1, keepdims=True) + EPS) * again_ref[...]
    ).astype(BF16)
    for load in loads[:5]:
        load.wait()

    def project(w):
        return jnp.dot(normed, w[...], preferred_element_type=F32).astype(BF16).astype(F32)

    q1, q2, k1, k2 = project(q1_v), project(q2_v), project(k1_v), project(k2_v)
    new_values[...] = project(vw_v)
    zero = jnp.zeros((seqs, half), F32)
    queries[...] = jnp.zeros_like(queries)
    kparts = []
    for h in range(heads):
        cut = slice(h * half, (h + 1) * half)
        kparts += [k1[:, cut], k2[:, cut]]
        for p, q in ((0, q1), (1, q2)):
            parts = [zero] * (2 * heads)
            parts[2 * h + p] = q[:, cut]
            queries[:, 4 * p + h, :] = jnp.concatenate(parts, axis=-1)
    own_keys[...] = jnp.concatenate(kparts, axis=-1)

    position = lax.broadcasted_iota(jnp.int32, (8, length), 1)
    row = lax.broadcasted_iota(jnp.int32, (8, width), 0)
    mine = row == lax.broadcasted_iota(jnp.int32, (8, width), 1) // head
    map_row = lax.broadcasted_iota(jnp.int32, (8, 1), 0)
    lam = jnp.zeros((8, 1), F32)
    for h in range(heads):
        lam = jnp.where(map_row == h, lam_ref[h], lam)
    hgain = jnp.concatenate([hgain_ref[...]] * heads, axis=-1)

    def group_step(g, carry):
        for j in range(GROUP):
            for copy in fetch(g * GROUP + j):
                copy.wait()
        for j in range(GROUP):
            s = g * GROUP + j
            raw[j] = lax.dot_general(
                queries[s].astype(BF16), kbuf[s], (((1,), (1,)), ((), ())), preferred_element_type=F32
            )
        own_ws = []
        for j in range(GROUP):
            s = g * GROUP + j
            own = jnp.sum(queries[s] * own_keys[pl.ds(s, 1), :], axis=-1, keepdims=True) * scale
            scores = jnp.where(position < lengths_ref[s], raw[j] * scale, -jnp.inf)
            top = jnp.maximum(jnp.max(scores, axis=-1, keepdims=True), own)
            raised = jnp.exp(scores - top)
            own_raised = jnp.exp(own - top)
            total = jnp.sum(raised, axis=-1, keepdims=True) + own_raised
            inv = 1.0 / total
            probs = raised * inv
            own_probs = own_raised * inv
            weights_v[j] = (probs - lam * pltpu.roll(probs, 4, 0)).astype(BF16)
            own_b = jnp.broadcast_to(own_probs, (8, 128))
            own_ws.append((own_b - lam * pltpu.roll(own_b, 4, 0)).astype(BF16).astype(F32)[:, :1])
        outs = []
        for j in range(GROUP):
            s = g * GROUP + j
            count = lengths_ref[s]
            pieces = [
                jnp.where(c * PIECE < count, vbuf[s, c * PIECE:(c + 1) * PIECE, :], jnp.zeros((PIECE, width), BF16))
                for c in range(length // PIECE)
            ]
            outs.append(jnp.dot(weights_v[j], jnp.concatenate(pieces, axis=0), preferred_element_type=F32))
        for j in range(GROUP):
            s = g * GROUP + j
            out = outs[j] + own_ws[j] * new_values[pl.ds(s, 1), :]
            out = jnp.where(mine, out, 0.0)
            mean_sq = jnp.sum(out * out, axis=-1, keepdims=True) * (1.0 / head)
            out = out * lax.rsqrt(mean_sq + EPS)
            attended[pl.ds(s, 1), :] = jnp.sum(out, axis=0, keepdims=True) * hgain
        return carry

    lax.fori_loop(0, seqs // GROUP, group_step, 0)
    loads[5].wait()
    part_ref[...] = jnp.dot(
        attended[...].astype(BF16), ow_v[...], preferred_element_type=F32
    ).reshape(part_ref.shape).astype(part_ref.dtype)


def attend(
    tokens, lengths, cache_keys, cache_values, attn_gain, q1w, q2w, k1w, k2w, vw, lam, hgain, out_w, out_dtype, parts
):
    seqs, length, width = cache_keys.shape
    heads = lam.shape[0]
    vm = pl.BlockSpec(memory_space=pltpu.VMEM)
    anyspace = pl.BlockSpec(memory_space=pltpu.HBM)
    scratch = [pltpu.VMEM(cache_keys.shape, BF16), pltpu.VMEM(cache_values.shape, BF16)]
    scratch += [pltpu.VMEM(w.shape, BF16) for w in (q1w, q2w, k1w, k2w, vw, out_w)]
    scratch += [
        pltpu.VMEM((seqs, 8, width), F32),
        pltpu.VMEM((seqs, width), F32),
        pltpu.VMEM((seqs, width), F32),
        pltpu.VMEM((seqs, width), F32),
        pltpu.VMEM((GROUP, 8, length), F32),
        pltpu.VMEM((GROUP, 8, length), BF16),
        pltpu.SMEM((seqs,), jnp.int32),
        pltpu.VMEM(tokens.shape, BF16),
        pltpu.VMEM((1, tokens.shape[1]), F32),
        pltpu.VMEM((1, hgain.shape[0]), F32),
        pltpu.SemaphoreType.DMA((seqs,)),
        pltpu.SemaphoreType.DMA((seqs,)),
        pltpu.SemaphoreType.DMA((6,)),
        pltpu.SemaphoreType.DMA((4,)),
    ]
    return pl.pallas_call(
        functools.partial(attend_kernel, heads),
        out_shape=jax.ShapeDtypeStruct((parts, seqs // parts, out_w.shape[1]), out_dtype),
        in_specs=[pl.BlockSpec(memory_space=pltpu.SMEM)] + [anyspace] * 12,
        out_specs=vm,
        scratch_shapes=scratch,
        compiler_params=pltpu.CompilerParams(vmem_limit_bytes=VMEM_BYTES),
        name="attend",
    )(
        lam, lengths, tokens, attn_gain.reshape(1, -1), hgain.reshape(1, -1),
        cache_keys, cache_values, q1w, q2w, k1w, k2w, vw, out_w,
    )


MESH = pl.DeviceIdType.MESH


def rms_scale(rows, gain):
    mean_sq = jnp.mean(rows * rows, axis=-1, keepdims=True)
    return rows * lax.rsqrt(mean_sq + EPS) * gain


def exact_dot(a, b):
    return jnp.dot(a, b, precision=lax.Precision.HIGHEST, preferred_element_type=F32)


def where_is(shape, dim):
    return lax.broadcasted_iota(jnp.int32, shape, dim)


def turned_dot(a, b, left, right):
    return lax.dot_general(
        a, b, (((left,), (right,)), ((), ())), precision=lax.Precision.HIGHEST, preferred_element_type=F32
    )


def route_tables(routes, logits, slots, capacity):
    top, seqs = routes.shape
    n = seqs * top
    routes = routes.astype(F32)
    spread = turned_dot(routes, (where_is((top, n), 1) % top == where_is((top, n), 0)).astype(F32), 0, 0)
    row = jnp.sum(jnp.where(where_is((seqs, n), 1) // top == where_is((seqs, n), 0), spread, 0.0), axis=0, keepdims=True)
    owner = (where_is((n, seqs), 0) // top == where_is((n, seqs), 1)).astype(F32)
    pick = where_is((n, top), 0) % top == where_is((n, top), 1)
    col = jnp.sum(jnp.where(pick, turned_dot(owner, routes, 1, 1), 0.0), axis=1, keepdims=True)
    same = row == col
    i, j = where_is((n, n), 0), where_is((n, n), 1)
    rank_col = jnp.sum((same & (j < i)).astype(F32), axis=1, keepdims=True)
    rank_row = jnp.sum((same & (i < j)).astype(F32), axis=0, keepdims=True)
    slot_row = row * capacity + rank_row
    return slot_row, lambda: combine_table(logits, col, rank_col, owner, pick, slots, capacity)


def combine_table(logits, col, rank_col, owner, pick, slots, capacity):
    n, seqs = owner.shape
    top = n // seqs
    slot_col = col * capacity + rank_col
    raised = jnp.exp(logits - jnp.max(logits, axis=0, keepdims=True))
    weights = raised / jnp.sum(raised, axis=0, keepdims=True)
    weight_col = jnp.sum(jnp.where(pick, turned_dot(owner, weights, 1, 1), 0.0), axis=1, keepdims=True)
    hit = where_is((n, slots), 1).astype(F32) == slot_col
    member = (where_is((seqs, n), 1) // top == where_is((seqs, n), 0)).astype(F32)
    combine = exact_dot(member, jnp.where(hit, weight_col, 0.0))
    return combine


def flip(index, mask):
    bit = 1
    out = index
    while bit <= mask:
        if mask & bit:
            out = out + (1 - 2 * lax.rem(index // bit, 2)) * bit
        bit *= 2
    return out


def layer_kernel(
    heads,
    groups,
    parts,
    capacity,
    lam_hbm,
    lengths_hbm,
    tokens_hbm,
    again_hbm,
    hgain_hbm,
    fgain_hbm,
    routes_hbm,
    logits_hbm,
    keys_hbm,
    values_hbm,
    q1_hbm,
    q2_hbm,
    k1_hbm,
    k2_hbm,
    vw_hbm,
    ow_hbm,
    gate_hbm,
    up_hbm,
    down_hbm,
    out_ref,
    kbuf,
    vbuf,
    q1_v,
    q2_v,
    k1_v,
    k2_v,
    vw_v,
    ow_v,
    gate_v,
    up_v,
    down_v,
    queries,
    own_keys,
    new_values,
    attended,
    raw,
    weights_v,
    lam_ref,
    lengths_ref,
    tokens_ref,
    again_ref,
    hgain_ref,
    fgain_ref,
    routes_ref,
    logits_ref,
    wide_v,
    part_f,
    part_b,
    rs_buf,
    kept,
    slot_buf,
    combine_v,
    xbuf,
    hbuf,
    resbuf,
    ret,
    ksem,
    vsem,
    wsem,
    ssem,
    snd,
    rs_r,
    sl_r,
    ag_r,
    far_r,
    near_r,
    relay_r,
    tail_r,
    hy_r,
    hc_r,
    hd_r,
    re_r,
):
    e, t = lax.axis_index("ep"), lax.axis_index("tp")
    seqs, length, width = kbuf.shape
    head = width // heads
    half = head // 2
    scale = half ** (-0.5)
    owned = gate_v.shape[0]
    columns = out_ref.shape[1]
    pieces = seqs // GROUP
    top = routes_ref.shape[0]
    n = seqs * top
    block = owned * capacity
    per = groups * capacity
    twin = t + 1 - 2 * lax.rem(t, 2)
    across = lax.rem(t + 2, parts)

    smalls = (
        (lengths_hbm, lengths_ref), (tokens_hbm, tokens_ref), (again_hbm, again_ref), (hgain_hbm, hgain_ref),
        (fgain_hbm, fgain_ref), (routes_hbm, routes_ref), (logits_hbm, logits_ref), (lam_hbm, lam_ref),
    )
    smalls = [pltpu.make_async_copy(src, dst, ssem.at[i]) for i, (src, dst) in enumerate(smalls)]
    for small in smalls:
        small.start()
    weights = [(q1_hbm, q1_v), (q2_hbm, q2_v), (k1_hbm, k1_v), (k2_hbm, k2_v), (vw_hbm, vw_v), (ow_hbm, ow_v)]
    for j in range(owned):
        for src, dst in ((gate_hbm, gate_v), (up_hbm, up_v), (down_hbm, down_v)):
            weights.append((src.at[j], dst.at[j]))
    loads = [pltpu.make_async_copy(src, dst, wsem.at[i]) for i, (src, dst) in enumerate(weights)]
    for load in loads[:5]:
        load.start()

    def arrived(ref, sem):
        pltpu.make_async_copy(ref, ref, sem).wait()

    def fetch_keys(s):
        return pltpu.make_async_copy(keys_hbm.at[s], kbuf.at[s], ksem.at[s // GROUP])

    def fetch_values(s):
        return pltpu.make_async_copy(values_hbm.at[s], vbuf.at[s], vsem.at[s // GROUP])

    def start_all(fetch, g):
        if g < pieces:
            for j in range(GROUP):
                fetch(g * GROUP + j).start()

    for j in range(GROUP // 2):
        fetch_keys(j).start()

    barrier = pltpu.get_barrier_semaphore()
    for k in range(1, parts):
        pl.semaphore_signal(barrier, inc=1, device_id=(e, lax.rem(t + k, parts)), device_id_type=MESH)
    for m in range(1, groups):
        pl.semaphore_signal(barrier, inc=1, device_id=(flip(e, m), t), device_id_type=MESH)

    def remote(src, dst, s_sem, r_sem, device):
        return pltpu.make_async_remote_copy(
            src_ref=src, dst_ref=dst, send_sem=s_sem, recv_sem=r_sem, device_id=device, device_id_type=MESH
        )

    def send(src, dst, s_sem, r_sem, device):
        copy = remote(src, dst, snd.at[s_sem], r_sem, device)
        copy.start()
        return copy

    for i in (1, 2):
        smalls[i].wait()
    for j in range(GROUP // 2, GROUP):
        fetch_keys(j).start()
    start_all(fetch_values, 0)
    loads[5].start()
    wide = tokens_ref[...].astype(F32)
    wide_v[...] = wide
    own_columns = pl.ds(pl.multiple_of(t * columns, columns), columns)
    kept[...] = wide_v[:, own_columns].reshape(kept.shape)
    normed = (
        wide * lax.rsqrt(jnp.mean(wide * wide, axis=-1, keepdims=True) + EPS) * again_ref[...]
    ).astype(BF16)
    for load in loads[:5]:
        load.wait()
    start_all(fetch_keys, 1)

    def project(w):
        return jnp.dot(normed, w[...], preferred_element_type=F32).astype(BF16).astype(F32)

    q1, q2, k1, k2 = project(q1_v), project(q2_v), project(k1_v), project(k2_v)
    new_values[...] = project(vw_v)
    zero = jnp.zeros((seqs, half), F32)
    queries[...] = jnp.zeros_like(queries)
    kparts = []
    for h in range(heads):
        cut = slice(h * half, (h + 1) * half)
        kparts += [k1[:, cut], k2[:, cut]]
        for p, q in ((0, q1), (1, q2)):
            mixed = [zero] * (2 * heads)
            mixed[2 * h + p] = q[:, cut]
            queries[:, 4 * p + h, :] = jnp.concatenate(mixed, axis=-1)
    own_keys[...] = jnp.concatenate(kparts, axis=-1)

    for i in (0, 3, 4, 5, 6, 7):
        smalls[i].wait()
    fgain = fgain_ref[:, own_columns]
    position = lax.broadcasted_iota(jnp.int32, (8, length), 1)
    row = lax.broadcasted_iota(jnp.int32, (8, width), 0)
    mine = row == lax.broadcasted_iota(jnp.int32, (8, width), 1) // head
    map_row = lax.broadcasted_iota(jnp.int32, (8, 1), 0)
    lam = jnp.zeros((8, 1), F32)
    for h in range(heads):
        lam = jnp.where(map_row == h, lam_ref[h], lam)
    hgain = jnp.concatenate([hgain_ref[...]] * heads, axis=-1)

    def attention(g):
        arrived(kbuf.at[pl.ds(g * GROUP, GROUP)], ksem.at[g])
        start_all(fetch_values, g + 1)
        for j in range(GROUP):
            s = g * GROUP + j
            raw[j] = lax.dot_general(
                queries[s].astype(BF16), kbuf[s], (((1,), (1,)), ((), ())), preferred_element_type=F32
            )
        own_ws = []
        for j in range(GROUP):
            s = g * GROUP + j
            own = jnp.sum(queries[s] * own_keys[pl.ds(s, 1), :], axis=-1, keepdims=True) * scale
            scores = jnp.where(position < lengths_ref[s], raw[j] * scale, -jnp.inf)
            highest = jnp.maximum(jnp.max(scores, axis=-1, keepdims=True), own)
            raised = jnp.exp(scores - highest)
            own_raised = jnp.exp(own - highest)
            total = jnp.sum(raised, axis=-1, keepdims=True) + own_raised
            inv = 1.0 / total
            probs = raised * inv
            own_probs = own_raised * inv
            weights_v[j] = (probs - lam * pltpu.roll(probs, 4, 0)).astype(BF16)
            own_b = jnp.broadcast_to(own_probs, (8, 128))
            own_ws.append((own_b - lam * pltpu.roll(own_b, 4, 0)).astype(BF16).astype(F32)[:, :1])
        arrived(vbuf.at[pl.ds(g * GROUP, GROUP)], vsem.at[g])
        start_all(fetch_keys, g + 2)
        outs = [
            jnp.dot(weights_v[j], vbuf[g * GROUP + j], preferred_element_type=F32) for j in range(GROUP)
        ]
        for j in range(GROUP):
            s = g * GROUP + j
            out = outs[j] + own_ws[j] * new_values[pl.ds(s, 1), :]
            out = jnp.where(mine, out, 0.0)
            mean_sq = jnp.sum(out * out, axis=-1, keepdims=True) * (1.0 / head)
            out = out * lax.rsqrt(mean_sq + EPS)
            attended[pl.ds(s, 1), :] = jnp.sum(out, axis=0, keepdims=True) * hgain

    def send_partials(g):
        heads_out = attended[g * GROUP:(g + 1) * GROUP, :].astype(BF16)
        partial = jnp.dot(heads_out, ow_v[...], preferred_element_type=F32)
        for q in range(parts):
            cut = partial[:, q * columns:(q + 1) * columns]
            part_f[q] = cut
            part_b[g, q] = cut.astype(BF16)
        for k in range(1, parts):
            peer = lax.rem(t + k, parts)
            send(part_b.at[g, peer], rs_buf.at[g, k - 1], 0, rs_r.at[g], (e, peer))
        kept[g] = kept[g] + part_f[t]

    gather, far, tail = {}, {}, {}
    opposite = lax.rem(twin + 2, parts)
    last = pieces - 1

    def late(g, m):
        return g == last and m >= groups // 2

    def forward(g, m):
        view = xbuf.at[g, t, flip(e, m)]
        far[g, m] = send(view, view, 3, far_r.at[g, m], (e, across))
        if late(g, m):
            tail[m] = send(view, view, 3, tail_r.at[m], (e, opposite))
        send(view, view, 3, near_r.at[0], (e, twin))

    def relay_rows(g):
        for m in range(groups):
            far[g, m].wait_recv()
            if not late(g, m):
                view = xbuf.at[g, across, flip(e, m)]
                send(view, view, 3, relay_r.at[int(g == last)], (e, twin))

    def send_rows(g):
        arrived(rs_buf.at[g], rs_r.at[g])
        total = kept[g]
        for k in range(1, parts):
            total = total + rs_buf[g, k - 1].astype(F32)
        kept[g] = total
        xbuf[g, t, e] = (total * fgain).astype(BF16)
        view = xbuf.at[g, t, e]
        for m in range(groups - 1, 0, -1):
            gather[g, m] = send(view, view, 2, ag_r.at[g, m - 1], (flip(e, m), t))
        forward(g, 0)

    def forward_rows(g, sources):
        for m in sources:
            gather[g, m].wait_recv()
            forward(g, m)

    close, distant = range(1, groups // 2), range(groups // 2, groups)

    for g in range(pieces):
        attention(g)
        if g == 0:
            pl.semaphore_wait(barrier, parts + groups - 2)
            loads[5].wait()
        send_partials(g)
        if g >= 1:
            send_rows(g - 1)
        if g >= 3:
            forward_rows(g - 3, distant)
        if g >= 2:
            forward_rows(g - 2, close)

    fetches = loads[6:]
    third = owned
    for load in fetches[:third]:
        load.start()
    slot_row, later = route_tables(routes_ref[...], logits_ref[...], groups * block, capacity)
    slot_buf[e] = jnp.broadcast_to(slot_row, (8, n))
    for m in range(groups - 1, 0, -1):
        send(slot_buf.at[e], slot_buf.at[e], 1, sl_r.at[0], (flip(e, m), t))
    share = later()
    for i in range(3):
        coarse = share.astype(BF16)
        combine_v[i * seqs:(i + 1) * seqs, :] = coarse
        share = share - coarse.astype(F32)
    forward_rows(last - 2, distant)
    send_rows(last)
    for load in fetches[third:]:
        load.start()
    for g in range(last - 1):
        relay_rows(g)
    forward_rows(last - 1, close)
    forward_rows(last - 1, distant)
    forward_rows(last, close)
    forward_rows(last, distant)
    arrived(slot_buf.at[pl.ds(0, groups - 1)], sl_r.at[0])
    base = e * block
    local = (where_is((block, n), 0) + base).astype(F32)
    tokens_all = groups * seqs
    token = where_is((n, tokens_all), 0) // top
    spot_row = token // GROUP * (groups * GROUP) + token % GROUP
    place = []
    for b in range(groups):
        chosen = (slot_buf[b][:1, :] == local).astype(BF16)
        spot = (where_is((n, tokens_all), 1) == spot_row + b * GROUP).astype(BF16)
        placed = jnp.dot(chosen, spot, preferred_element_type=F32)
        place.append(placed.reshape(owned, 1, capacity, tokens_all))
    dispatch = jnp.concatenate(place, axis=1).reshape(groups * block, tokens_all).astype(BF16)

    relay_rows(last - 1)
    relay_rows(last)
    arrived(xbuf.at[:, 0], near_r.at[0])
    arrived(xbuf.at[pl.ds(0, last), 0], relay_r.at[0])
    arrived(xbuf.at[last, 0, pl.ds(0, groups // 2)], relay_r.at[1])
    for copy in tail.values():
        copy.wait_recv()

    lines, squares = [], jnp.zeros((groups * block, columns), F32)
    for q in range(parts):
        rows = xbuf[:, q].astype(F32).reshape(tokens_all, columns).astype(BF16)
        picked = jnp.dot(dispatch, rows, preferred_element_type=F32)
        lines.append(picked.astype(BF16))
        plain = picked * (1.0 / fgain_ref[:, q * columns:(q + 1) * columns])
        squares = squares + plain * plain
    lines = jnp.concatenate(lines, axis=-1)
    mean_sq = jnp.sum(squares, axis=-1, keepdims=True) * (1.0 / (columns * parts))
    row_scale = lax.rsqrt(mean_sq + EPS)
    hfar, hnear = [], []
    for j in range(owned):
        for i in range(2):
            loads[6 + 3 * j + i].wait()
        line = lines[j * per:(j + 1) * per]
        line_scale = row_scale[j * per:(j + 1) * per]
        gate = jnp.minimum(jnp.dot(line, gate_v[j], preferred_element_type=F32) * line_scale, LIMIT)
        up = jnp.clip(jnp.dot(line, up_v[j], preferred_element_type=F32) * line_scale, -LIMIT, LIMIT)
        hbuf[j, t] = ((up + 1.0) * gate * jax.nn.sigmoid(ALPHA * gate)).astype(BF16)
        view = hbuf.at[j, t]
        hfar.append(send(view, view, 4, hy_r.at[j], (e, across)))
        if j == 0:
            hrelay = [send(view, view, 4, hd_r.at[j], (e, opposite))]
        hnear.append(send(view, view, 4, hc_r.at[j], (e, twin)))
    deep = hbuf.shape[3]
    for j in range(owned + 1):
        if j < owned:
            hfar[j].wait_recv()
            theirs = hbuf.at[j, across]
            if j:
                hrelay.append(send(theirs, theirs, 4, hd_r.at[j], (e, twin)))
        if j == 0:
            continue
        i = j - 1
        hnear[i].wait_recv()
        hrelay[i].wait_recv()
        loads[6 + 3 * i + 2].wait()
        result = jnp.zeros((per, columns), F32)
        for q in range(parts):
            result += jnp.dot(hbuf[i, q], down_v[i, q * deep:(q + 1) * deep, :], preferred_element_type=F32)
        resbuf[i] = result.reshape(groups, capacity, columns).astype(BF16)
        for m in range(groups - 1, 0, -1):
            peer = flip(e, m)
            send(resbuf.at[i, peer], ret.at[e, i], 5, re_r.at[0], (peer, t))
        ret[e, i] = resbuf[i, e]
    arrived(ret.at[pl.ds(0, groups - 1)], re_r.at[0])
    results = ret[...].astype(F32).reshape(groups * block, columns).astype(BF16)
    moe = jnp.dot(combine_v[...], results, preferred_element_type=F32)
    moe = moe[:seqs] + moe[seqs:2 * seqs] + moe[2 * seqs:]
    out_ref[...] = (kept[...].reshape(seqs, columns) + moe).astype(out_ref.dtype)
    arrived(part_b.at[:, pl.ds(0, parts - 1)], snd.at[0])
    arrived(slot_buf.at[pl.ds(0, groups - 1)], snd.at[1])
    arrived(xbuf.at[:, 0, pl.ds(0, groups - 1)], snd.at[2])
    arrived(xbuf.at[:, pl.ds(0, parts - 1)], snd.at[3])
    arrived(hbuf.at[:, pl.ds(0, parts - 1)], snd.at[4])
    arrived(resbuf.at[:, pl.ds(0, groups - 1)], snd.at[5])


def layer(
    tokens, lengths, cache_keys, cache_values, attn_gain, q1w, q2w, k1w, k2w, vw, lam, hgain, out_w,
    ffn_gain, routes, logits, gate_w, up_w, down_w, groups, parts, capacity,
):
    seqs, length, width = cache_keys.shape
    heads = lam.shape[0]
    owned, _, deep = gate_w.shape
    columns = down_w.shape[2]
    per = groups * capacity
    pieces = seqs // GROUP
    full = tokens.shape[1]
    routes, logits = routes.T, logits.T
    anyspace = pl.BlockSpec(memory_space=pltpu.HBM)
    scratch = [pltpu.VMEM(cache_keys.shape, BF16), pltpu.VMEM(cache_values.shape, BF16)]
    scratch += [pltpu.VMEM(w.shape, BF16) for w in (q1w, q2w, k1w, k2w, vw, out_w, gate_w, up_w, down_w)]
    scratch += [
        pltpu.VMEM((seqs, 8, width), F32),
        pltpu.VMEM((seqs, width), F32),
        pltpu.VMEM((seqs, width), F32),
        pltpu.VMEM((seqs, width), F32),
        pltpu.VMEM((GROUP, 8, length), F32),
        pltpu.VMEM((GROUP, 8, length), BF16),
        pltpu.SMEM(lam.shape, F32),
        pltpu.SMEM((seqs,), jnp.int32),
        pltpu.VMEM(tokens.shape, BF16),
        pltpu.VMEM((1, full), F32),
        pltpu.VMEM((1, hgain.shape[0]), F32),
        pltpu.VMEM((1, full), F32),
        pltpu.VMEM(routes.shape, routes.dtype),
        pltpu.VMEM(logits.shape, F32),
        pltpu.VMEM(tokens.shape, F32),
        pltpu.VMEM((parts, GROUP, columns), F32),
        pltpu.VMEM((pieces, parts, GROUP, columns), BF16),
        pltpu.VMEM((pieces, parts - 1, GROUP, columns), BF16),
        pltpu.VMEM((pieces, GROUP, columns), F32),
        pltpu.VMEM((groups, 8, routes.size), F32),
        pltpu.VMEM((3 * seqs, owned * per), BF16),
        pltpu.VMEM((pieces, parts, groups, GROUP, columns), BF16),
        pltpu.VMEM((owned, parts, per, deep), BF16),
        pltpu.VMEM((owned, groups, capacity, columns), BF16),
        pltpu.VMEM((groups, owned, capacity, columns), BF16),
    ]
    dma = lambda *shape: [pltpu.SemaphoreType.DMA(shape)]
    scratch += dma(pieces) * 2 + dma(6 + 3 * owned) + dma(8)
    scratch += dma(6) + dma(pieces) + dma(1) + dma(pieces, groups - 1)
    scratch += dma(pieces, groups) + dma(1) + dma(2) + dma(groups) + dma(owned) * 3 + dma(1)
    return pl.pallas_call(
        functools.partial(layer_kernel, heads, groups, parts, capacity),
        out_shape=pltpu.VMEM((seqs, columns), BF16),
        in_specs=[anyspace] * 19,
        out_specs=pl.BlockSpec(memory_space=pltpu.VMEM),
        scratch_shapes=scratch,
        compiler_params=pltpu.CompilerParams(
            collective_id=0, has_side_effects=True, vmem_limit_bytes=LAYER_BYTES
        ),
        name="layer",
    )(
        lam, lengths, tokens, attn_gain.reshape(1, -1), hgain.reshape(1, -1), ffn_gain.reshape(1, -1),
        routes, logits, cache_keys, cache_values, q1w, q2w, k1w, k2w, vw, out_w, gate_w, up_w, down_w,
    )


def slot_tables(routes, weights, expert_ids, capacity):
    blocks, seqs, top = routes.shape
    flat = routes.reshape(blocks, seqs * top)
    order = jnp.arange(seqs * top, dtype=jnp.int32)
    same = (flat[:, None, :] == flat[:, :, None]) & (order[None, None, :] < order[None, :, None])
    rank = jnp.sum(same.astype(jnp.int32), axis=2)
    match = flat[:, :, None] == expert_ids[None, None, :]
    hit = rank[:, :, None] == jnp.arange(capacity, dtype=jnp.int32)[None, None, :]
    table = (match[:, :, :, None] & hit[:, :, None, :]).astype(jnp.float32)
    table = table.reshape(blocks, seqs, top, expert_ids.shape[0], capacity)
    dispatch = jnp.sum(table, axis=2)
    combine = jnp.sum(table * weights[:, :, :, None, None], axis=2)
    return (dispatch, combine)


def run_experts(buffer, gate_w, up_w, down_w):
    gate = jnp.einsum("bjcd,jdf->bjcf", buffer, gate_w, preferred_element_type=jnp.float32)
    up = jnp.einsum("bjcd,jdf->bjcf", buffer, up_w, preferred_element_type=jnp.float32)
    bound_gate = jnp.minimum(gate, LIMIT)
    bound_up = jnp.clip(up, -LIMIT, LIMIT)
    hidden = ((bound_up + 1.0) * bound_gate * jax.nn.sigmoid(ALPHA * bound_gate)).astype(
        jnp.bfloat16
    )
    total = jnp.einsum(
        "bjcf,jfd->bjcd",
        lax.all_gather(hidden, "tp", axis=3, tiled=True),
        down_w,
        preferred_element_type=jnp.float32,
    )
    return total.astype(jnp.bfloat16)


def per_device(
    tokens,
    lengths,
    cache_keys,
    cache_values,
    attn_gain,
    q_first_w,
    q_second_w,
    k_first_w,
    k_second_w,
    value_w,
    mix_lambda,
    head_gain,
    out_w,
    ffn_gain,
    routes,
    route_logits,
    gate_w,
    up_w,
    down_w,
):
    groups, parts = lax.axis_size("ep"), lax.axis_size("tp")
    owned = gate_w.shape[0]
    seqs, top = routes.shape
    capacity = max(2, 2 * seqs * top // (owned * groups))
    fused = (
        parts == 4 and seqs % GROUP == 0 and seqs >= 4 * GROUP and capacity % 8 == 0 and seqs * top % 128 == 0 and groups & (groups - 1) == 0
    )
    if fused:
        return layer(
            tokens, lengths, cache_keys, cache_values, attn_gain, q_first_w, q_second_w, k_first_w, k_second_w,
            value_w, mix_lambda, head_gain, out_w, ffn_gain, routes, route_logits, gate_w, up_w, down_w,
            groups, parts, capacity,
        )
    partial_value = attend(
        tokens,
        lengths,
        cache_keys,
        cache_values,
        attn_gain,
        q_first_w,
        q_second_w,
        k_first_w,
        k_second_w,
        value_w,
        mix_lambda,
        head_gain,
        out_w,
        F32,
        1,
    )
    partial_value = partial_value.reshape(tokens.shape)
    wide = tokens.astype(F32)
    columns = wide.shape[1] // lax.axis_size("tp")
    start = lax.axis_index("tp") * columns
    summed = lax.psum(partial_value, "tp")
    after = wide + summed
    full_in = rms_scale(after, ffn_gain).astype(jnp.bfloat16)
    kept = lax.dynamic_slice_in_dim(after, start, columns, 1)
    weights = jax.nn.softmax(route_logits, axis=-1)
    expert_ids = jnp.arange(owned * groups, dtype=jnp.int32)
    dispatch, combine = slot_tables(routes[None], weights[None], expert_ids, capacity)
    buffer = jnp.einsum(
        "bsjc,bsd->bjcd",
        dispatch.astype(jnp.bfloat16),
        full_in[None],
        preferred_element_type=jnp.float32,
    ).astype(jnp.bfloat16)
    buffer = buffer.reshape(groups, owned, capacity, -1)
    arrived = lax.all_to_all(buffer, "ep", split_axis=0, concat_axis=0, tiled=True)
    results = run_experts(arrived, gate_w, up_w, down_w)
    returned = lax.all_to_all(results, "ep", split_axis=0, concat_axis=0, tiled=True).reshape(
        1, groups * owned, capacity, -1
    )
    moe = jnp.einsum(
        "bsjc,bjcd->bsd", combine, returned.astype(jnp.float32), precision=lax.Precision.HIGHEST
    )[0]
    return (kept + moe).astype(jnp.bfloat16)


def solution(mesh):
    return jax.shard_map(
        per_device,
        mesh=mesh,
        in_specs=(
            P("ep", None),
            P("ep"),
            P("ep", None, "tp"),
            P("ep", None, "tp"),
            P(),
            P(None, "tp"),
            P(None, "tp"),
            P(None, "tp"),
            P(None, "tp"),
            P(None, "tp"),
            P("tp"),
            P(),
            P("tp", None),
            P(),
            P("ep", None),
            P("ep", None),
            P("ep", None, "tp"),
            P("ep", None, "tp"),
            P("ep", None, "tp"),
        ),
        out_specs=P("ep", "tp"),
        check_vma=False,
    )
```

```python
import functools

import jax
import jax.numpy as jnp
from jax import lax
from jax.experimental import pallas as pl
from jax.experimental.pallas import tpu as pltpu
from jax.sharding import PartitionSpec as P

EPS = 1e-06
LIMIT = 7.0
ALPHA = 1.702
PIECE = 128
GROUP = 8
VMEM_BYTES = 67043328
LAYER_BYTES = 60 * 1024 * 1024
F32 = jnp.float32
BF16 = jnp.bfloat16


def attend_kernel(
    heads,
    lam_ref,
    lengths_hbm,
    tokens_hbm,
    again_hbm,
    hgain_hbm,
    keys_hbm,
    values_hbm,
    q1_hbm,
    q2_hbm,
    k1_hbm,
    k2_hbm,
    vw_hbm,
    ow_hbm,
    part_ref,
    kbuf,
    vbuf,
    q1_v,
    q2_v,
    k1_v,
    k2_v,
    vw_v,
    ow_v,
    queries,
    own_keys,
    new_values,
    attended,
    raw,
    weights_v,
    lengths_ref,
    tokens_ref,
    again_ref,
    hgain_ref,
    ksem,
    vsem,
    wsem,
    ssem,
):
    smalls = ((lengths_hbm, lengths_ref), (tokens_hbm, tokens_ref), (again_hbm, again_ref), (hgain_hbm, hgain_ref))
    smalls = [pltpu.make_async_copy(src, dst, ssem.at[i]) for i, (src, dst) in enumerate(smalls)]
    for small in smalls:
        small.start()
    seqs, length, width = kbuf.shape
    head = width // heads
    half = head // 2
    scale = half ** (-0.5)
    weights = ((q1_hbm, q1_v), (q2_hbm, q2_v), (k1_hbm, k1_v), (k2_hbm, k2_v), (vw_hbm, vw_v), (ow_hbm, ow_v))
    loads = [pltpu.make_async_copy(src, dst, wsem.at[i]) for i, (src, dst) in enumerate(weights)]
    for load in loads[:5]:
        load.start()

    def fetch(s):
        rows = pl.multiple_of((lengths_ref[s] + (PIECE - 1)) // PIECE * PIECE, PIECE)
        return (
            pltpu.make_async_copy(keys_hbm.at[s, pl.ds(0, rows)], kbuf.at[s, pl.ds(0, rows)], ksem.at[s]),
            pltpu.make_async_copy(values_hbm.at[s, pl.ds(0, rows)], vbuf.at[s, pl.ds(0, rows)], vsem.at[s]),
        )

    def start(s, carry):
        a, b = fetch(s)
        a.start()
        b.start()
        return carry

    smalls[0].wait()
    lax.fori_loop(0, seqs, start, 0)
    loads[5].start()
    for small in smalls[1:]:
        small.wait()

    wide = tokens_ref[...].astype(F32)
    normed = (
        wide * lax.rsqrt(jnp.mean(wide * wide, axis=-1, keepdims=True) + EPS) * again_ref[...]
    ).astype(BF16)
    for load in loads[:5]:
        load.wait()

    def project(w):
        return jnp.dot(normed, w[...], preferred_element_type=F32).astype(BF16).astype(F32)

    q1, q2, k1, k2 = project(q1_v), project(q2_v), project(k1_v), project(k2_v)
    new_values[...] = project(vw_v)
    zero = jnp.zeros((seqs, half), F32)
    queries[...] = jnp.zeros_like(queries)
    kparts = []
    for h in range(heads):
        cut = slice(h * half, (h + 1) * half)
        kparts += [k1[:, cut], k2[:, cut]]
        for p, q in ((0, q1), (1, q2)):
            parts = [zero] * (2 * heads)
            parts[2 * h + p] = q[:, cut]
            queries[:, 4 * p + h, :] = jnp.concatenate(parts, axis=-1)
    own_keys[...] = jnp.concatenate(kparts, axis=-1)

    position = lax.broadcasted_iota(jnp.int32, (8, length), 1)
    row = lax.broadcasted_iota(jnp.int32, (8, width), 0)
    mine = row == lax.broadcasted_iota(jnp.int32, (8, width), 1) // head
    map_row = lax.broadcasted_iota(jnp.int32, (8, 1), 0)
    lam = jnp.zeros((8, 1), F32)
    for h in range(heads):
        lam = jnp.where(map_row == h, lam_ref[h], lam)
    hgain = jnp.concatenate([hgain_ref[...]] * heads, axis=-1)

    def group_step(g, carry):
        for j in range(GROUP):
            for copy in fetch(g * GROUP + j):
                copy.wait()
        for j in range(GROUP):
            s = g * GROUP + j
            raw[j] = lax.dot_general(
                queries[s].astype(BF16), kbuf[s], (((1,), (1,)), ((), ())), preferred_element_type=F32
            )
        own_ws = []
        for j in range(GROUP):
            s = g * GROUP + j
            own = jnp.sum(queries[s] * own_keys[pl.ds(s, 1), :], axis=-1, keepdims=True) * scale
            scores = jnp.where(position < lengths_ref[s], raw[j] * scale, -jnp.inf)
            top = jnp.maximum(jnp.max(scores, axis=-1, keepdims=True), own)
            raised = jnp.exp(scores - top)
            own_raised = jnp.exp(own - top)
            total = jnp.sum(raised, axis=-1, keepdims=True) + own_raised
            inv = 1.0 / total
            probs = raised * inv
            own_probs = own_raised * inv
            weights_v[j] = (probs - lam * pltpu.roll(probs, 4, 0)).astype(BF16)
            own_b = jnp.broadcast_to(own_probs, (8, 128))
            own_ws.append((own_b - lam * pltpu.roll(own_b, 4, 0)).astype(BF16).astype(F32)[:, :1])
        outs = []
        for j in range(GROUP):
            s = g * GROUP + j
            count = lengths_ref[s]
            pieces = [
                jnp.where(c * PIECE < count, vbuf[s, c * PIECE:(c + 1) * PIECE, :], jnp.zeros((PIECE, width), BF16))
                for c in range(length // PIECE)
            ]
            outs.append(jnp.dot(weights_v[j], jnp.concatenate(pieces, axis=0), preferred_element_type=F32))
        for j in range(GROUP):
            s = g * GROUP + j
            out = outs[j] + own_ws[j] * new_values[pl.ds(s, 1), :]
            out = jnp.where(mine, out, 0.0)
            mean_sq = jnp.sum(out * out, axis=-1, keepdims=True) * (1.0 / head)
            out = out * lax.rsqrt(mean_sq + EPS)
            attended[pl.ds(s, 1), :] = jnp.sum(out, axis=0, keepdims=True) * hgain
        return carry

    lax.fori_loop(0, seqs // GROUP, group_step, 0)
    loads[5].wait()
    part_ref[...] = jnp.dot(
        attended[...].astype(BF16), ow_v[...], preferred_element_type=F32
    ).reshape(part_ref.shape).astype(part_ref.dtype)


def attend(
    tokens, lengths, cache_keys, cache_values, attn_gain, q1w, q2w, k1w, k2w, vw, lam, hgain, out_w, out_dtype, parts
):
    seqs, length, width = cache_keys.shape
    heads = lam.shape[0]
    vm = pl.BlockSpec(memory_space=pltpu.VMEM)
    anyspace = pl.BlockSpec(memory_space=pltpu.HBM)
    scratch = [pltpu.VMEM(cache_keys.shape, BF16), pltpu.VMEM(cache_values.shape, BF16)]
    scratch += [pltpu.VMEM(w.shape, BF16) for w in (q1w, q2w, k1w, k2w, vw, out_w)]
    scratch += [
        pltpu.VMEM((seqs, 8, width), F32),
        pltpu.VMEM((seqs, width), F32),
        pltpu.VMEM((seqs, width), F32),
        pltpu.VMEM((seqs, width), F32),
        pltpu.VMEM((GROUP, 8, length), F32),
        pltpu.VMEM((GROUP, 8, length), BF16),
        pltpu.SMEM((seqs,), jnp.int32),
        pltpu.VMEM(tokens.shape, BF16),
        pltpu.VMEM((1, tokens.shape[1]), F32),
        pltpu.VMEM((1, hgain.shape[0]), F32),
        pltpu.SemaphoreType.DMA((seqs,)),
        pltpu.SemaphoreType.DMA((seqs,)),
        pltpu.SemaphoreType.DMA((6,)),
        pltpu.SemaphoreType.DMA((4,)),
    ]
    return pl.pallas_call(
        functools.partial(attend_kernel, heads),
        out_shape=jax.ShapeDtypeStruct((parts, seqs // parts, out_w.shape[1]), out_dtype),
        in_specs=[pl.BlockSpec(memory_space=pltpu.SMEM)] + [anyspace] * 12,
        out_specs=vm,
        scratch_shapes=scratch,
        compiler_params=pltpu.CompilerParams(vmem_limit_bytes=VMEM_BYTES),
        name="attend",
    )(
        lam, lengths, tokens, attn_gain.reshape(1, -1), hgain.reshape(1, -1),
        cache_keys, cache_values, q1w, q2w, k1w, k2w, vw, out_w,
    )


MESH = pl.DeviceIdType.MESH


def rms_scale(rows, gain):
    mean_sq = jnp.mean(rows * rows, axis=-1, keepdims=True)
    return rows * lax.rsqrt(mean_sq + EPS) * gain


def exact_dot(a, b):
    return jnp.dot(a, b, precision=lax.Precision.HIGHEST, preferred_element_type=F32)


def where_is(shape, dim):
    return lax.broadcasted_iota(jnp.int32, shape, dim)


def turned_dot(a, b, left, right):
    return lax.dot_general(
        a, b, (((left,), (right,)), ((), ())), precision=lax.Precision.HIGHEST, preferred_element_type=F32
    )


def route_tables(routes, logits, slots, capacity):
    top, seqs = routes.shape
    n = seqs * top
    routes = routes.astype(F32)
    spread = turned_dot(routes, (where_is((top, n), 1) % top == where_is((top, n), 0)).astype(F32), 0, 0)
    row = jnp.sum(jnp.where(where_is((seqs, n), 1) // top == where_is((seqs, n), 0), spread, 0.0), axis=0, keepdims=True)
    owner = (where_is((n, seqs), 0) // top == where_is((n, seqs), 1)).astype(F32)
    pick = where_is((n, top), 0) % top == where_is((n, top), 1)
    col = jnp.sum(jnp.where(pick, turned_dot(owner, routes, 1, 1), 0.0), axis=1, keepdims=True)
    same = row == col
    i, j = where_is((n, n), 0), where_is((n, n), 1)
    rank_col = jnp.sum((same & (j < i)).astype(F32), axis=1, keepdims=True)
    rank_row = jnp.sum((same & (i < j)).astype(F32), axis=0, keepdims=True)
    slot_row = row * capacity + rank_row
    return slot_row, lambda: combine_table(logits, col, rank_col, owner, pick, slots, capacity)


def combine_table(logits, col, rank_col, owner, pick, slots, capacity):
    n, seqs = owner.shape
    top = n // seqs
    slot_col = col * capacity + rank_col
    raised = jnp.exp(logits - jnp.max(logits, axis=0, keepdims=True))
    weights = raised / jnp.sum(raised, axis=0, keepdims=True)
    weight_col = jnp.sum(jnp.where(pick, turned_dot(owner, weights, 1, 1), 0.0), axis=1, keepdims=True)
    hit = where_is((n, slots), 1).astype(F32) == slot_col
    member = (where_is((seqs, n), 1) // top == where_is((seqs, n), 0)).astype(F32)
    combine = exact_dot(member, jnp.where(hit, weight_col, 0.0))
    return combine


def flip(index, mask):
    bit = 1
    out = index
    while bit <= mask:
        if mask & bit:
            out = out + (1 - 2 * lax.rem(index // bit, 2)) * bit
        bit *= 2
    return out


def layer_kernel(
    heads,
    groups,
    parts,
    capacity,
    lam_hbm,
    lengths_hbm,
    tokens_hbm,
    again_hbm,
    hgain_hbm,
    fgain_hbm,
    routes_hbm,
    logits_hbm,
    keys_hbm,
    values_hbm,
    q1_hbm,
    q2_hbm,
    k1_hbm,
    k2_hbm,
    vw_hbm,
    ow_hbm,
    gate_hbm,
    up_hbm,
    down_hbm,
    out_ref,
    kbuf,
    vbuf,
    q1_v,
    q2_v,
    k1_v,
    k2_v,
    vw_v,
    ow_v,
    gate_v,
    up_v,
    down_v,
    queries,
    own_keys,
    new_values,
    attended,
    raw,
    weights_v,
    lam_ref,
    lengths_ref,
    tokens_ref,
    again_ref,
    hgain_ref,
    fgain_ref,
    routes_ref,
    logits_ref,
    wide_v,
    part_f,
    part_b,
    rs_buf,
    kept,
    slot_buf,
    combine_v,
    dispatch_v,
    lines_v,
    xbuf,
    hbuf,
    resbuf,
    ret,
    ksem,
    vsem,
    wsem,
    ssem,
    snd,
    rs_r,
    sl_r,
    own_r,
    wide_r,
    join_r,
    hy_r,
    hc_r,
    hd_r,
    re_r,
):
    e, t = lax.axis_index("ep"), lax.axis_index("tp")
    seqs, length, width = kbuf.shape
    head = width // heads
    half = head // 2
    scale = half ** (-0.5)
    owned = gate_v.shape[0]
    columns = out_ref.shape[1]
    pieces = seqs // GROUP
    top = routes_ref.shape[0]
    n = seqs * top
    block = owned * capacity
    per = groups * capacity
    twin = t + 1 - 2 * lax.rem(t, 2)
    across = lax.rem(t + 2, parts)

    smalls = (
        (lengths_hbm, lengths_ref), (tokens_hbm, tokens_ref), (again_hbm, again_ref), (hgain_hbm, hgain_ref),
        (fgain_hbm, fgain_ref), (routes_hbm, routes_ref), (logits_hbm, logits_ref), (lam_hbm, lam_ref),
    )
    smalls = [pltpu.make_async_copy(src, dst, ssem.at[i]) for i, (src, dst) in enumerate(smalls)]
    for small in smalls:
        small.start()
    weights = [(q1_hbm, q1_v), (q2_hbm, q2_v), (k1_hbm, k1_v), (k2_hbm, k2_v), (vw_hbm, vw_v), (ow_hbm, ow_v)]
    for j in range(owned):
        for src, dst in ((gate_hbm, gate_v), (up_hbm, up_v), (down_hbm, down_v)):
            weights.append((src.at[j], dst.at[j]))
    loads = [pltpu.make_async_copy(src, dst, wsem.at[i]) for i, (src, dst) in enumerate(weights)]
    for load in loads[:5]:
        load.start()

    def arrived(ref, sem):
        pltpu.make_async_copy(ref, ref, sem).wait()

    def fetch_keys(s):
        return pltpu.make_async_copy(keys_hbm.at[s], kbuf.at[s], ksem.at[s // GROUP])

    def fetch_values(s):
        return pltpu.make_async_copy(values_hbm.at[s], vbuf.at[s], vsem.at[s // GROUP])

    def start_all(fetch, g):
        if g < pieces:
            for j in range(GROUP):
                fetch(g * GROUP + j).start()

    for j in range(GROUP // 2):
        fetch_keys(j).start()

    barrier = pltpu.get_barrier_semaphore()
    for k in range(1, parts):
        pl.semaphore_signal(barrier, inc=1, device_id=(e, lax.rem(t + k, parts)), device_id_type=MESH)
    for m in range(1, groups):
        for side in (t, across):
            pl.semaphore_signal(barrier, inc=1, device_id=(flip(e, m), side), device_id_type=MESH)

    def remote(src, dst, s_sem, r_sem, device):
        return pltpu.make_async_remote_copy(
            src_ref=src, dst_ref=dst, send_sem=s_sem, recv_sem=r_sem, device_id=device, device_id_type=MESH
        )

    def send(src, dst, s_sem, r_sem, device):
        copy = remote(src, dst, snd.at[s_sem], r_sem, device)
        copy.start()
        return copy

    for i in (1, 2):
        smalls[i].wait()
    for j in range(GROUP // 2, GROUP):
        fetch_keys(j).start()
    wide = tokens_ref[...].astype(F32)
    wide_v[...] = wide
    own_columns = pl.ds(pl.multiple_of(t * columns, columns), columns)
    kept[...] = wide_v[:, own_columns].reshape(kept.shape)
    normed = (
        wide * lax.rsqrt(jnp.mean(wide * wide, axis=-1, keepdims=True) + EPS) * again_ref[...]
    ).astype(BF16)
    for i in (4, 5, 6):
        smalls[i].wait()
    slot_row, later = route_tables(routes_ref[...], logits_ref[...], groups * block, capacity)
    slot_buf[e] = jnp.broadcast_to(slot_row, (8, n))
    share = later()
    for i in range(3):
        coarse = share.astype(BF16)
        combine_v[i * seqs:(i + 1) * seqs, :] = coarse
        share = share - coarse.astype(F32)
    for load in loads[:5]:
        load.wait()
    start_all(fetch_values, 0)
    loads[5].start()
    start_all(fetch_keys, 1)

    def project(w):
        return jnp.dot(normed, w[...], preferred_element_type=F32).astype(BF16).astype(F32)

    q1, q2, k1, k2 = project(q1_v), project(q2_v), project(k1_v), project(k2_v)
    new_values[...] = project(vw_v)
    zero = jnp.zeros((seqs, half), F32)
    queries[...] = jnp.zeros_like(queries)
    kparts = []
    for h in range(heads):
        cut = slice(h * half, (h + 1) * half)
        kparts += [k1[:, cut], k2[:, cut]]
        for p, q in ((0, q1), (1, q2)):
            mixed = [zero] * (2 * heads)
            mixed[2 * h + p] = q[:, cut]
            queries[:, 4 * p + h, :] = jnp.concatenate(mixed, axis=-1)
    own_keys[...] = jnp.concatenate(kparts, axis=-1)

    for i in (0, 3, 7):
        smalls[i].wait()
    fgain = fgain_ref[:, own_columns]
    position = lax.broadcasted_iota(jnp.int32, (8, length), 1)
    row = lax.broadcasted_iota(jnp.int32, (8, width), 0)
    mine = row == lax.broadcasted_iota(jnp.int32, (8, width), 1) // head
    map_row = lax.broadcasted_iota(jnp.int32, (8, 1), 0)
    lam = jnp.zeros((8, 1), F32)
    for h in range(heads):
        lam = jnp.where(map_row == h, lam_ref[h], lam)
    hgain = jnp.concatenate([hgain_ref[...]] * heads, axis=-1)

    def attention(g):
        arrived(kbuf.at[pl.ds(g * GROUP, GROUP)], ksem.at[g])
        start_all(fetch_values, g + 1)
        for j in range(GROUP):
            s = g * GROUP + j
            raw[j] = lax.dot_general(
                queries[s].astype(BF16), kbuf[s], (((1,), (1,)), ((), ())), preferred_element_type=F32
            )
        own_ws = []
        for j in range(GROUP):
            s = g * GROUP + j
            own = jnp.sum(queries[s] * own_keys[pl.ds(s, 1), :], axis=-1, keepdims=True) * scale
            scores = jnp.where(position < lengths_ref[s], raw[j] * scale, -jnp.inf)
            highest = jnp.maximum(jnp.max(scores, axis=-1, keepdims=True), own)
            raised = jnp.exp(scores - highest)
            own_raised = jnp.exp(own - highest)
            total = jnp.sum(raised, axis=-1, keepdims=True) + own_raised
            inv = 1.0 / total
            probs = raised * inv
            own_probs = own_raised * inv
            weights_v[j] = (probs - lam * pltpu.roll(probs, 4, 0)).astype(BF16)
            own_b = jnp.broadcast_to(own_probs, (8, 128))
            own_ws.append((own_b - lam * pltpu.roll(own_b, 4, 0)).astype(BF16).astype(F32)[:, :1])
        arrived(vbuf.at[pl.ds(g * GROUP, GROUP)], vsem.at[g])
        start_all(fetch_keys, g + 2)
        outs = [
            jnp.dot(weights_v[j], vbuf[g * GROUP + j], preferred_element_type=F32) for j in range(GROUP)
        ]
        for j in range(GROUP):
            s = g * GROUP + j
            out = outs[j] + own_ws[j] * new_values[pl.ds(s, 1), :]
            out = jnp.where(mine, out, 0.0)
            mean_sq = jnp.sum(out * out, axis=-1, keepdims=True) * (1.0 / head)
            out = out * lax.rsqrt(mean_sq + EPS)
            attended[pl.ds(s, 1), :] = jnp.sum(out, axis=0, keepdims=True) * hgain

    def send_partials(g):
        heads_out = attended[g * GROUP:(g + 1) * GROUP, :].astype(BF16)
        partial = jnp.dot(heads_out, ow_v[...], preferred_element_type=F32)
        for q in range(parts):
            cut = partial[:, q * columns:(q + 1) * columns]
            part_f[q] = cut
            part_b[g, q] = cut.astype(BF16)
        for k in range(1, parts):
            peer = lax.rem(t + k, parts)
            send(part_b.at[g, peer], rs_buf.at[g, k - 1], 0, rs_r.at[g], (e, peer))
        kept[g] = kept[g] + part_f[t]

    own, last = {}, pieces - 1
    opposite = lax.rem(twin + 2, parts)

    def send_rows(g):
        arrived(rs_buf.at[g], rs_r.at[g])
        total = kept[g]
        for k in range(1, parts):
            total = total + rs_buf[g, k - 1].astype(F32)
        kept[g] = total
        xbuf[g, t, e] = (total * fgain).astype(BF16)
        view = xbuf.at[g, t, e]
        for m in range(groups - 1, 0, -1):
            for side in (t, across):
                send(view, view, 2, wide_r.at[g], (flip(e, m), side))
        own[g] = send(view, view, 3, own_r.at[g], (e, across))

    def join_rows(g):
        own[g].wait_recv()
        arrived(xbuf.at[g, pl.ds(0, 2), pl.ds(0, groups - 1)], wide_r.at[g])
        for side in (t, across):
            view = xbuf.at[g, side]
            send(view, view, 6, join_r.at[g], (e, twin))

    for g in range(pieces):
        attention(g)
        if g == 0:
            pl.semaphore_wait(barrier, parts - 1 + 2 * (groups - 1))
            loads[5].wait()
        send_partials(g)
        if g == 0:
            for m in range(groups - 1, 0, -1):
                send(slot_buf.at[e], slot_buf.at[e], 1, sl_r.at[0], (flip(e, m), t))
        if g >= 1:
            send_rows(g - 1)

    fetches = loads[6:]
    third = owned
    for load in fetches[:third]:
        load.start()
    arrived(slot_buf.at[pl.ds(0, groups - 1)], sl_r.at[0])
    base = e * block
    local = (where_is((block, n), 0) + base).astype(F32)
    chosen = [(slot_buf[b][:1, :] == local).astype(BF16) for b in range(groups)]

    def dispatch_from(first, count):
        wide_n = count * groups * GROUP
        token = where_is((n, wide_n), 0) // top
        spot_row = (token // GROUP - first) * (groups * GROUP) + token % GROUP
        place = []
        for b in range(groups):
            spot = (where_is((n, wide_n), 1) == spot_row + b * GROUP).astype(BF16)
            placed = jnp.dot(chosen[b], spot, preferred_element_type=F32)
            place.append(placed.reshape(owned, 1, capacity, wide_n))
        return jnp.concatenate(place, axis=1).reshape(groups * block, wide_n).astype(BF16)

    def rows_from(first, count, q):
        rows = xbuf[first:first + count, q].astype(F32)
        return rows.reshape(count * groups * GROUP, columns).astype(BF16)

    dispatch_first = dispatch_from(0, last)
    dispatch_v[...] = dispatch_from(last, 1)
    send_rows(last)
    for load in fetches[third:]:
        load.start()
    for g in range(last):
        join_rows(g)
    for g in range(last):
        arrived(xbuf.at[g, pl.ds(0, 2)], join_r.at[g])
    for q in range(parts):
        lines_v[:, q * columns:(q + 1) * columns] = jnp.dot(
            dispatch_first, rows_from(0, last, q), preferred_element_type=F32
        )
    join_rows(last)
    arrived(xbuf.at[last, pl.ds(0, 2)], join_r.at[last])
    late = [rows_from(last, 1, q) for q in range(parts)]
    unscale = 1.0 / fgain_ref[...]
    hfar, hnear = [None], [None]
    half_rows = groups // 2 * capacity
    home = e // (groups // 2) * (groups // 2)
    away = groups // 2 - home
    for j in range(owned):
        for i in range(2):
            loads[6 + 3 * j + i].wait()
        picked = jnp.concatenate(
            [jnp.dot(dispatch_v[j * per:(j + 1) * per, :], rows, preferred_element_type=F32) for rows in late], axis=-1
        ) + lines_v[j * per:(j + 1) * per, :]
        line = picked.astype(BF16)
        plain = picked * unscale
        mean_sq = jnp.sum(plain * plain, axis=-1, keepdims=True) * (1.0 / (columns * parts))
        line_scale = lax.rsqrt(mean_sq + EPS)
        gate = jnp.minimum(jnp.dot(line, gate_v[j], preferred_element_type=F32) * line_scale, LIMIT)
        up = jnp.clip(jnp.dot(line, up_v[j], preferred_element_type=F32) * line_scale, -LIMIT, LIMIT)
        hbuf[j, t] = ((up + 1.0) * gate * jax.nn.sigmoid(ALPHA * gate)).astype(BF16)
        if j == 0:
            halves = []
            for i, base_row in enumerate((away, home)):
                view = hbuf.at[j, t, pl.ds(pl.multiple_of(base_row * capacity, half_rows), half_rows)]
                halves.append([
                    send(view, view, 4, hy_r.at[i * owned], (e, across)),
                    send(view, view, 4, hd_r.at[i * owned], (e, opposite)),
                    send(view, view, 4, hc_r.at[i * owned], (e, twin)),
                ])
            continue
        view = hbuf.at[j, t]
        hfar.append(send(view, view, 4, hy_r.at[j], (e, across)))
        hnear.append(send(view, view, 4, hc_r.at[j], (e, twin)))
    deep = hbuf.shape[3]
    hrelay = [None]
    loads[6 + 2].wait()
    for i, base_row in enumerate((away, home)):
        for copy in halves[i]:
            copy.wait_recv()
        result = jnp.zeros((half_rows, columns), F32)
        cut = pl.ds(pl.multiple_of(base_row * capacity, half_rows), half_rows)
        for q in range(parts):
            result += jnp.dot(hbuf[0, q, cut, :], down_v[0, q * deep:(q + 1) * deep, :], preferred_element_type=F32)
        resbuf[0, pl.ds(base_row, groups // 2)] = result.reshape(groups // 2, capacity, columns).astype(BF16)
        for m in (range(groups - 1, groups // 2 - 1, -1) if i == 0 else range(groups // 2 - 1, 0, -1)):
            peer = flip(e, m)
            send(resbuf.at[0, peer], ret.at[e, 0], 5, re_r.at[0], (peer, t))
    ret[e, 0] = resbuf[0, e]
    for j in range(1, owned + 1):
        if j < owned:
            hfar[j].wait_recv()
            theirs = hbuf.at[j, across]
            hrelay.append(send(theirs, theirs, 4, hd_r.at[j], (e, twin)))
        if j == 1:
            continue
        i = j - 1
        hnear[i].wait_recv()
        hrelay[i].wait_recv()
        loads[6 + 3 * i + 2].wait()
        result = jnp.zeros((per, columns), F32)
        for q in range(parts):
            result += jnp.dot(hbuf[i, q], down_v[i, q * deep:(q + 1) * deep, :], preferred_element_type=F32)
        resbuf[i] = result.reshape(groups, capacity, columns).astype(BF16)
        for m in range(groups - 1, 0, -1):
            peer = flip(e, m)
            send(resbuf.at[i, peer], ret.at[e, i], 5, re_r.at[0], (peer, t))
        ret[e, i] = resbuf[i, e]
    arrived(ret.at[pl.ds(0, groups - 1)], re_r.at[0])
    results = ret[...].astype(F32).reshape(groups * block, columns).astype(BF16)
    moe = jnp.dot(combine_v[...], results, preferred_element_type=F32)
    moe = moe[:seqs] + moe[seqs:2 * seqs] + moe[2 * seqs:]
    out_ref[...] = (kept[...].reshape(seqs, columns) + moe).astype(out_ref.dtype)
    arrived(part_b.at[:, pl.ds(0, parts - 1)], snd.at[0])
    arrived(slot_buf.at[pl.ds(0, groups - 1)], snd.at[1])
    arrived(xbuf.at[:, pl.ds(0, 2), pl.ds(0, groups - 1)], snd.at[2])
    arrived(xbuf.at[:, 0, 0], snd.at[3])
    arrived(xbuf.at[:, pl.ds(0, 2)], snd.at[6])
    arrived(hbuf.at[:, pl.ds(0, parts - 1)], snd.at[4])
    arrived(resbuf.at[:, pl.ds(0, groups - 1)], snd.at[5])


def layer(
    tokens, lengths, cache_keys, cache_values, attn_gain, q1w, q2w, k1w, k2w, vw, lam, hgain, out_w,
    ffn_gain, routes, logits, gate_w, up_w, down_w, groups, parts, capacity,
):
    seqs, length, width = cache_keys.shape
    heads = lam.shape[0]
    owned, _, deep = gate_w.shape
    columns = down_w.shape[2]
    per = groups * capacity
    pieces = seqs // GROUP
    full = tokens.shape[1]
    routes, logits = routes.T, logits.T
    anyspace = pl.BlockSpec(memory_space=pltpu.HBM)
    scratch = [pltpu.VMEM(cache_keys.shape, BF16), pltpu.VMEM(cache_values.shape, BF16)]
    scratch += [pltpu.VMEM(w.shape, BF16) for w in (q1w, q2w, k1w, k2w, vw, out_w, gate_w, up_w, down_w)]
    scratch += [
        pltpu.VMEM((seqs, 8, width), F32),
        pltpu.VMEM((seqs, width), F32),
        pltpu.VMEM((seqs, width), F32),
        pltpu.VMEM((seqs, width), F32),
        pltpu.VMEM((GROUP, 8, length), F32),
        pltpu.VMEM((GROUP, 8, length), BF16),
        pltpu.SMEM(lam.shape, F32),
        pltpu.SMEM((seqs,), jnp.int32),
        pltpu.VMEM(tokens.shape, BF16),
        pltpu.VMEM((1, full), F32),
        pltpu.VMEM((1, hgain.shape[0]), F32),
        pltpu.VMEM((1, full), F32),
        pltpu.VMEM(routes.shape, routes.dtype),
        pltpu.VMEM(logits.shape, F32),
        pltpu.VMEM(tokens.shape, F32),
        pltpu.VMEM((parts, GROUP, columns), F32),
        pltpu.VMEM((pieces, parts, GROUP, columns), BF16),
        pltpu.VMEM((pieces, parts - 1, GROUP, columns), BF16),
        pltpu.VMEM((pieces, GROUP, columns), F32),
        pltpu.VMEM((groups, 8, routes.size), F32),
        pltpu.VMEM((3 * seqs, owned * per), BF16),
        pltpu.VMEM((owned * per, groups * GROUP), BF16),
        pltpu.VMEM((owned * per, full), F32),
        pltpu.VMEM((pieces, parts, groups, GROUP, columns), BF16),
        pltpu.VMEM((owned, parts, per, deep), BF16),
        pltpu.VMEM((owned, groups, capacity, columns), BF16),
        pltpu.VMEM((groups, owned, capacity, columns), BF16),
    ]
    dma = lambda *shape: [pltpu.SemaphoreType.DMA(shape)]
    scratch += dma(pieces) * 2 + dma(6 + 3 * owned) + dma(8)
    scratch += dma(7) + dma(pieces) + dma(1) + dma(pieces) * 3 + dma(owned + 1) * 3 + dma(1)
    return pl.pallas_call(
        functools.partial(layer_kernel, heads, groups, parts, capacity),
        out_shape=pltpu.VMEM((seqs, columns), BF16),
        in_specs=[anyspace] * 19,
        out_specs=pl.BlockSpec(memory_space=pltpu.VMEM),
        scratch_shapes=scratch,
        compiler_params=pltpu.CompilerParams(
            collective_id=0, has_side_effects=True, vmem_limit_bytes=LAYER_BYTES
        ),
        name="layer",
    )(
        lam, lengths, tokens, attn_gain.reshape(1, -1), hgain.reshape(1, -1), ffn_gain.reshape(1, -1),
        routes, logits, cache_keys, cache_values, q1w, q2w, k1w, k2w, vw, out_w, gate_w, up_w, down_w,
    )


def slot_tables(routes, weights, expert_ids, capacity):
    blocks, seqs, top = routes.shape
    flat = routes.reshape(blocks, seqs * top)
    order = jnp.arange(seqs * top, dtype=jnp.int32)
    same = (flat[:, None, :] == flat[:, :, None]) & (order[None, None, :] < order[None, :, None])
    rank = jnp.sum(same.astype(jnp.int32), axis=2)
    match = flat[:, :, None] == expert_ids[None, None, :]
    hit = rank[:, :, None] == jnp.arange(capacity, dtype=jnp.int32)[None, None, :]
    table = (match[:, :, :, None] & hit[:, :, None, :]).astype(jnp.float32)
    table = table.reshape(blocks, seqs, top, expert_ids.shape[0], capacity)
    dispatch = jnp.sum(table, axis=2)
    combine = jnp.sum(table * weights[:, :, :, None, None], axis=2)
    return (dispatch, combine)


def run_experts(buffer, gate_w, up_w, down_w):
    gate = jnp.einsum("bjcd,jdf->bjcf", buffer, gate_w, preferred_element_type=jnp.float32)
    up = jnp.einsum("bjcd,jdf->bjcf", buffer, up_w, preferred_element_type=jnp.float32)
    bound_gate = jnp.minimum(gate, LIMIT)
    bound_up = jnp.clip(up, -LIMIT, LIMIT)
    hidden = ((bound_up + 1.0) * bound_gate * jax.nn.sigmoid(ALPHA * bound_gate)).astype(
        jnp.bfloat16
    )
    total = jnp.einsum(
        "bjcf,jfd->bjcd",
        lax.all_gather(hidden, "tp", axis=3, tiled=True),
        down_w,
        preferred_element_type=jnp.float32,
    )
    return total.astype(jnp.bfloat16)


def per_device(
    tokens,
    lengths,
    cache_keys,
    cache_values,
    attn_gain,
    q_first_w,
    q_second_w,
    k_first_w,
    k_second_w,
    value_w,
    mix_lambda,
    head_gain,
    out_w,
    ffn_gain,
    routes,
    route_logits,
    gate_w,
    up_w,
    down_w,
):
    groups, parts = lax.axis_size("ep"), lax.axis_size("tp")
    owned = gate_w.shape[0]
    seqs, top = routes.shape
    capacity = max(2, 2 * seqs * top // (owned * groups))
    fused = (
        parts == 4 and seqs % GROUP == 0 and seqs >= 4 * GROUP and capacity % 8 == 0 and seqs * top % 128 == 0 and groups & (groups - 1) == 0
    )
    if fused:
        return layer(
            tokens, lengths, cache_keys, cache_values, attn_gain, q_first_w, q_second_w, k_first_w, k_second_w,
            value_w, mix_lambda, head_gain, out_w, ffn_gain, routes, route_logits, gate_w, up_w, down_w,
            groups, parts, capacity,
        )
    partial_value = attend(
        tokens,
        lengths,
        cache_keys,
        cache_values,
        attn_gain,
        q_first_w,
        q_second_w,
        k_first_w,
        k_second_w,
        value_w,
        mix_lambda,
        head_gain,
        out_w,
        F32,
        1,
    )
    partial_value = partial_value.reshape(tokens.shape)
    wide = tokens.astype(F32)
    columns = wide.shape[1] // lax.axis_size("tp")
    start = lax.axis_index("tp") * columns
    summed = lax.psum(partial_value, "tp")
    after = wide + summed
    full_in = rms_scale(after, ffn_gain).astype(jnp.bfloat16)
    kept = lax.dynamic_slice_in_dim(after, start, columns, 1)
    weights = jax.nn.softmax(route_logits, axis=-1)
    expert_ids = jnp.arange(owned * groups, dtype=jnp.int32)
    dispatch, combine = slot_tables(routes[None], weights[None], expert_ids, capacity)
    buffer = jnp.einsum(
        "bsjc,bsd->bjcd",
        dispatch.astype(jnp.bfloat16),
        full_in[None],
        preferred_element_type=jnp.float32,
    ).astype(jnp.bfloat16)
    buffer = buffer.reshape(groups, owned, capacity, -1)
    arrived = lax.all_to_all(buffer, "ep", split_axis=0, concat_axis=0, tiled=True)
    results = run_experts(arrived, gate_w, up_w, down_w)
    returned = lax.all_to_all(results, "ep", split_axis=0, concat_axis=0, tiled=True).reshape(
        1, groups * owned, capacity, -1
    )
    moe = jnp.einsum(
        "bsjc,bjcd->bsd", combine, returned.astype(jnp.float32), precision=lax.Precision.HIGHEST
    )[0]
    return (kept + moe).astype(jnp.bfloat16)


def solution(mesh):
    return jax.shard_map(
        per_device,
        mesh=mesh,
        in_specs=(
            P("ep", None),
            P("ep"),
            P("ep", None, "tp"),
            P("ep", None, "tp"),
            P(),
            P(None, "tp"),
            P(None, "tp"),
            P(None, "tp"),
            P(None, "tp"),
            P(None, "tp"),
            P("tp"),
            P(),
            P("tp", None),
            P(),
            P("ep", None),
            P("ep", None),
            P("ep", None, "tp"),
            P("ep", None, "tp"),
            P("ep", None, "tp"),
        ),
        out_specs=P("ep", "tp"),
        check_vma=False,
    )
```

```python
import functools

import jax
import jax.numpy as jnp
from jax import lax
from jax.experimental import pallas as pl
from jax.experimental.pallas import tpu as pltpu
from jax.sharding import PartitionSpec as P

EPS = 1e-06
LIMIT = 7.0
ALPHA = 1.702
PIECE = 128
GROUP = 8
VMEM_BYTES = 67043328
LAYER_BYTES = 60 * 1024 * 1024
F32 = jnp.float32
BF16 = jnp.bfloat16


def attend_kernel(
    heads,
    lam_ref,
    lengths_hbm,
    tokens_hbm,
    again_hbm,
    hgain_hbm,
    keys_hbm,
    values_hbm,
    q1_hbm,
    q2_hbm,
    k1_hbm,
    k2_hbm,
    vw_hbm,
    ow_hbm,
    part_ref,
    kbuf,
    vbuf,
    q1_v,
    q2_v,
    k1_v,
    k2_v,
    vw_v,
    ow_v,
    queries,
    own_keys,
    new_values,
    attended,
    raw,
    weights_v,
    lengths_ref,
    tokens_ref,
    again_ref,
    hgain_ref,
    ksem,
    vsem,
    wsem,
    ssem,
):
    smalls = ((lengths_hbm, lengths_ref), (tokens_hbm, tokens_ref), (again_hbm, again_ref), (hgain_hbm, hgain_ref))
    smalls = [pltpu.make_async_copy(src, dst, ssem.at[i]) for i, (src, dst) in enumerate(smalls)]
    for small in smalls:
        small.start()
    seqs, length, width = kbuf.shape
    head = width // heads
    half = head // 2
    scale = half ** (-0.5)
    weights = ((q1_hbm, q1_v), (q2_hbm, q2_v), (k1_hbm, k1_v), (k2_hbm, k2_v), (vw_hbm, vw_v), (ow_hbm, ow_v))
    loads = [pltpu.make_async_copy(src, dst, wsem.at[i]) for i, (src, dst) in enumerate(weights)]
    for load in loads[:5]:
        load.start()

    def fetch(s):
        rows = pl.multiple_of((lengths_ref[s] + (PIECE - 1)) // PIECE * PIECE, PIECE)
        return (
            pltpu.make_async_copy(keys_hbm.at[s, pl.ds(0, rows)], kbuf.at[s, pl.ds(0, rows)], ksem.at[s]),
            pltpu.make_async_copy(values_hbm.at[s, pl.ds(0, rows)], vbuf.at[s, pl.ds(0, rows)], vsem.at[s]),
        )

    def start(s, carry):
        a, b = fetch(s)
        a.start()
        b.start()
        return carry

    smalls[0].wait()
    lax.fori_loop(0, seqs, start, 0)
    loads[5].start()
    for small in smalls[1:]:
        small.wait()

    wide = tokens_ref[...].astype(F32)
    normed = (
        wide * lax.rsqrt(jnp.mean(wide * wide, axis=-1, keepdims=True) + EPS) * again_ref[...]
    ).astype(BF16)
    for load in loads[:5]:
        load.wait()

    def project(w):
        return jnp.dot(normed, w[...], preferred_element_type=F32).astype(BF16).astype(F32)

    q1, q2, k1, k2 = project(q1_v), project(q2_v), project(k1_v), project(k2_v)
    new_values[...] = project(vw_v)
    zero = jnp.zeros((seqs, half), F32)
    queries[...] = jnp.zeros_like(queries)
    kparts = []
    for h in range(heads):
        cut = slice(h * half, (h + 1) * half)
        kparts += [k1[:, cut], k2[:, cut]]
        for p, q in ((0, q1), (1, q2)):
            parts = [zero] * (2 * heads)
            parts[2 * h + p] = q[:, cut]
            queries[:, 4 * p + h, :] = jnp.concatenate(parts, axis=-1)
    own_keys[...] = jnp.concatenate(kparts, axis=-1)

    position = lax.broadcasted_iota(jnp.int32, (8, length), 1)
    row = lax.broadcasted_iota(jnp.int32, (8, width), 0)
    mine = row == lax.broadcasted_iota(jnp.int32, (8, width), 1) // head
    map_row = lax.broadcasted_iota(jnp.int32, (8, 1), 0)
    lam = jnp.zeros((8, 1), F32)
    for h in range(heads):
        lam = jnp.where(map_row == h, lam_ref[h], lam)
    hgain = jnp.concatenate([hgain_ref[...]] * heads, axis=-1)

    def group_step(g, carry):
        for j in range(GROUP):
            for copy in fetch(g * GROUP + j):
                copy.wait()
        for j in range(GROUP):
            s = g * GROUP + j
            raw[j] = lax.dot_general(
                queries[s].astype(BF16), kbuf[s], (((1,), (1,)), ((), ())), preferred_element_type=F32
            )
        own_ws = []
        for j in range(GROUP):
            s = g * GROUP + j
            own = jnp.sum(queries[s] * own_keys[pl.ds(s, 1), :], axis=-1, keepdims=True) * scale
            scores = jnp.where(position < lengths_ref[s], raw[j] * scale, -jnp.inf)
            top = jnp.maximum(jnp.max(scores, axis=-1, keepdims=True), own)
            raised = jnp.exp(scores - top)
            own_raised = jnp.exp(own - top)
            total = jnp.sum(raised, axis=-1, keepdims=True) + own_raised
            inv = 1.0 / total
            probs = raised * inv
            own_probs = own_raised * inv
            weights_v[j] = (probs - lam * pltpu.roll(probs, 4, 0)).astype(BF16)
            own_b = jnp.broadcast_to(own_probs, (8, 128))
            own_ws.append((own_b - lam * pltpu.roll(own_b, 4, 0)).astype(BF16).astype(F32)[:, :1])
        outs = []
        for j in range(GROUP):
            s = g * GROUP + j
            count = lengths_ref[s]
            pieces = [
                jnp.where(c * PIECE < count, vbuf[s, c * PIECE:(c + 1) * PIECE, :], jnp.zeros((PIECE, width), BF16))
                for c in range(length // PIECE)
            ]
            outs.append(jnp.dot(weights_v[j], jnp.concatenate(pieces, axis=0), preferred_element_type=F32))
        for j in range(GROUP):
            s = g * GROUP + j
            out = outs[j] + own_ws[j] * new_values[pl.ds(s, 1), :]
            out = jnp.where(mine, out, 0.0)
            mean_sq = jnp.sum(out * out, axis=-1, keepdims=True) * (1.0 / head)
            out = out * lax.rsqrt(mean_sq + EPS)
            attended[pl.ds(s, 1), :] = jnp.sum(out, axis=0, keepdims=True) * hgain
        return carry

    lax.fori_loop(0, seqs // GROUP, group_step, 0)
    loads[5].wait()
    part_ref[...] = jnp.dot(
        attended[...].astype(BF16), ow_v[...], preferred_element_type=F32
    ).reshape(part_ref.shape).astype(part_ref.dtype)


def attend(
    tokens, lengths, cache_keys, cache_values, attn_gain, q1w, q2w, k1w, k2w, vw, lam, hgain, out_w, out_dtype, parts
):
    seqs, length, width = cache_keys.shape
    heads = lam.shape[0]
    vm = pl.BlockSpec(memory_space=pltpu.VMEM)
    anyspace = pl.BlockSpec(memory_space=pltpu.HBM)
    scratch = [pltpu.VMEM(cache_keys.shape, BF16), pltpu.VMEM(cache_values.shape, BF16)]
    scratch += [pltpu.VMEM(w.shape, BF16) for w in (q1w, q2w, k1w, k2w, vw, out_w)]
    scratch += [
        pltpu.VMEM((seqs, 8, width), F32),
        pltpu.VMEM((seqs, width), F32),
        pltpu.VMEM((seqs, width), F32),
        pltpu.VMEM((seqs, width), F32),
        pltpu.VMEM((GROUP, 8, length), F32),
        pltpu.VMEM((GROUP, 8, length), BF16),
        pltpu.SMEM((seqs,), jnp.int32),
        pltpu.VMEM(tokens.shape, BF16),
        pltpu.VMEM((1, tokens.shape[1]), F32),
        pltpu.VMEM((1, hgain.shape[0]), F32),
        pltpu.SemaphoreType.DMA((seqs,)),
        pltpu.SemaphoreType.DMA((seqs,)),
        pltpu.SemaphoreType.DMA((6,)),
        pltpu.SemaphoreType.DMA((4,)),
    ]
    return pl.pallas_call(
        functools.partial(attend_kernel, heads),
        out_shape=jax.ShapeDtypeStruct((parts, seqs // parts, out_w.shape[1]), out_dtype),
        in_specs=[pl.BlockSpec(memory_space=pltpu.SMEM)] + [anyspace] * 12,
        out_specs=vm,
        scratch_shapes=scratch,
        compiler_params=pltpu.CompilerParams(vmem_limit_bytes=VMEM_BYTES),
        name="attend",
    )(
        lam, lengths, tokens, attn_gain.reshape(1, -1), hgain.reshape(1, -1),
        cache_keys, cache_values, q1w, q2w, k1w, k2w, vw, out_w,
    )


MESH = pl.DeviceIdType.MESH


def rms_scale(rows, gain):
    mean_sq = jnp.mean(rows * rows, axis=-1, keepdims=True)
    return rows * lax.rsqrt(mean_sq + EPS) * gain


def exact_dot(a, b):
    return jnp.dot(a, b, precision=lax.Precision.HIGHEST, preferred_element_type=F32)


def where_is(shape, dim):
    return lax.broadcasted_iota(jnp.int32, shape, dim)


def turned_dot(a, b, left, right):
    return lax.dot_general(
        a, b, (((left,), (right,)), ((), ())), precision=lax.Precision.HIGHEST, preferred_element_type=F32
    )


def route_tables(routes, logits, slots, capacity):
    top, seqs = routes.shape
    n = seqs * top
    routes = routes.astype(F32)
    spread = turned_dot(routes, (where_is((top, n), 1) % top == where_is((top, n), 0)).astype(F32), 0, 0)
    row = jnp.sum(jnp.where(where_is((seqs, n), 1) // top == where_is((seqs, n), 0), spread, 0.0), axis=0, keepdims=True)
    owner = (where_is((n, seqs), 0) // top == where_is((n, seqs), 1)).astype(F32)
    pick = where_is((n, top), 0) % top == where_is((n, top), 1)
    col = jnp.sum(jnp.where(pick, turned_dot(owner, routes, 1, 1), 0.0), axis=1, keepdims=True)
    same = row == col
    i, j = where_is((n, n), 0), where_is((n, n), 1)
    rank_col = jnp.sum((same & (j < i)).astype(F32), axis=1, keepdims=True)
    rank_row = jnp.sum((same & (i < j)).astype(F32), axis=0, keepdims=True)
    slot_row = row * capacity + rank_row
    return slot_row, lambda: combine_table(logits, col, rank_col, owner, pick, slots, capacity)


def combine_table(logits, col, rank_col, owner, pick, slots, capacity):
    n, seqs = owner.shape
    top = n // seqs
    slot_col = col * capacity + rank_col
    raised = jnp.exp(logits - jnp.max(logits, axis=0, keepdims=True))
    weights = raised / jnp.sum(raised, axis=0, keepdims=True)
    weight_col = jnp.sum(jnp.where(pick, turned_dot(owner, weights, 1, 1), 0.0), axis=1, keepdims=True)
    hit = where_is((n, slots), 1).astype(F32) == slot_col
    member = (where_is((seqs, n), 1) // top == where_is((seqs, n), 0)).astype(F32)
    combine = exact_dot(member, jnp.where(hit, weight_col, 0.0))
    return combine


def flip(index, mask):
    bit = 1
    out = index
    while bit <= mask:
        if mask & bit:
            out = out + (1 - 2 * lax.rem(index // bit, 2)) * bit
        bit *= 2
    return out


def layer_kernel(
    heads,
    groups,
    parts,
    capacity,
    lam_hbm,
    lengths_hbm,
    tokens_hbm,
    again_hbm,
    hgain_hbm,
    fgain_hbm,
    routes_hbm,
    logits_hbm,
    keys_hbm,
    values_hbm,
    q1_hbm,
    q2_hbm,
    k1_hbm,
    k2_hbm,
    vw_hbm,
    ow_hbm,
    gate_hbm,
    up_hbm,
    down_hbm,
    out_ref,
    kbuf,
    vbuf,
    q1_v,
    q2_v,
    k1_v,
    k2_v,
    vw_v,
    ow_v,
    gate_v,
    up_v,
    down_v,
    queries,
    own_keys,
    new_values,
    attended,
    raw,
    weights_v,
    lam_ref,
    lengths_ref,
    tokens_ref,
    again_ref,
    hgain_ref,
    fgain_ref,
    routes_ref,
    logits_ref,
    wide_v,
    part_f,
    part_b,
    rs_buf,
    kept,
    slot_buf,
    combine_v,
    dispatch_v,
    lines_v,
    squares_v,
    gate_up,
    xbuf,
    hbuf,
    resbuf,
    ret,
    ksem,
    vsem,
    wsem,
    ssem,
    snd,
    rs_r,
    sl_r,
    own_r,
    wide_r,
    join_r,
    hy_r,
    hc_r,
    hd_r,
    re_r,
):
    e, t = lax.axis_index("ep"), lax.axis_index("tp")
    seqs, length, width = kbuf.shape
    head = width // heads
    half = head // 2
    scale = half ** (-0.5)
    owned = gate_v.shape[0]
    columns = out_ref.shape[1]
    pieces = seqs // GROUP
    top = routes_ref.shape[0]
    n = seqs * top
    block = owned * capacity
    per = groups * capacity
    twin = t + 1 - 2 * lax.rem(t, 2)
    across = lax.rem(t + 2, parts)

    smalls = (
        (lengths_hbm, lengths_ref), (tokens_hbm, tokens_ref), (again_hbm, again_ref), (hgain_hbm, hgain_ref),
        (fgain_hbm, fgain_ref), (routes_hbm, routes_ref), (logits_hbm, logits_ref), (lam_hbm, lam_ref),
    )
    smalls = [pltpu.make_async_copy(src, dst, ssem.at[i]) for i, (src, dst) in enumerate(smalls)]
    for small in smalls:
        small.start()
    weights = [(q1_hbm, q1_v), (q2_hbm, q2_v), (k1_hbm, k1_v), (k2_hbm, k2_v), (vw_hbm, vw_v), (ow_hbm, ow_v)]
    for j in range(owned):
        for src, dst in ((gate_hbm, gate_v), (up_hbm, up_v), (down_hbm, down_v)):
            weights.append((src.at[j], dst.at[j]))
    loads = [pltpu.make_async_copy(src, dst, wsem.at[i]) for i, (src, dst) in enumerate(weights)]
    for load in loads[:5]:
        load.start()

    def arrived(ref, sem):
        pltpu.make_async_copy(ref, ref, sem).wait()

    def fetch_keys(s):
        return pltpu.make_async_copy(keys_hbm.at[s], kbuf.at[s], ksem.at[pieces if s < GROUP // 2 else s // GROUP])

    def fetch_values(s):
        return pltpu.make_async_copy(values_hbm.at[s], vbuf.at[s], vsem.at[s // GROUP])

    def start_all(fetch, g):
        if g < pieces:
            for j in range(GROUP):
                fetch(g * GROUP + j).start()

    barrier = pltpu.get_barrier_semaphore()
    for k in range(1, parts):
        pl.semaphore_signal(barrier, inc=1, device_id=(e, lax.rem(t + k, parts)), device_id_type=MESH)
    for m in range(1, groups):
        for side in (t, across):
            pl.semaphore_signal(barrier, inc=1, device_id=(flip(e, m), side), device_id_type=MESH)

    def remote(src, dst, s_sem, r_sem, device):
        return pltpu.make_async_remote_copy(
            src_ref=src, dst_ref=dst, send_sem=s_sem, recv_sem=r_sem, device_id=device, device_id_type=MESH
        )

    def send(src, dst, s_sem, r_sem, device):
        copy = remote(src, dst, snd.at[s_sem], r_sem, device)
        copy.start()
        return copy

    for i in (1, 2):
        smalls[i].wait()
    start_all(fetch_keys, 0)
    wide = tokens_ref[...].astype(F32)
    wide_v[...] = wide
    own_columns = pl.ds(pl.multiple_of(t * columns, columns), columns)
    kept[...] = wide_v[:, own_columns].reshape(kept.shape)
    normed = (
        wide * lax.rsqrt(jnp.mean(wide * wide, axis=-1, keepdims=True) + EPS) * again_ref[...]
    ).astype(BF16)
    for i in (4, 5, 6):
        smalls[i].wait()
    slot_row, _ = route_tables(routes_ref[...], logits_ref[...], groups * block, capacity)
    slot_buf[e] = jnp.broadcast_to(slot_row, (8, n))
    for load in loads[:5]:
        load.wait()
    start_all(fetch_values, 0)
    loads[5].start()

    def project(w):
        return jnp.dot(normed, w[...], preferred_element_type=F32).astype(BF16).astype(F32)

    q1, q2, k1, k2 = project(q1_v), project(q2_v), project(k1_v), project(k2_v)
    new_values[...] = project(vw_v)
    zero = jnp.zeros((seqs, half), F32)
    queries[...] = jnp.zeros_like(queries)
    kparts = []
    for h in range(heads):
        cut = slice(h * half, (h + 1) * half)
        kparts += [k1[:, cut], k2[:, cut]]
        for p, q in ((0, q1), (1, q2)):
            mixed = [zero] * (2 * heads)
            mixed[2 * h + p] = q[:, cut]
            queries[:, 4 * p + h, :] = jnp.concatenate(mixed, axis=-1)
    own_keys[...] = jnp.concatenate(kparts, axis=-1)

    for i in (0, 3, 7):
        smalls[i].wait()
    fgain = fgain_ref[:, own_columns]
    position = lax.broadcasted_iota(jnp.int32, (8, length), 1)
    row = lax.broadcasted_iota(jnp.int32, (8, width), 0)
    mine = row == lax.broadcasted_iota(jnp.int32, (8, width), 1) // head
    map_row = lax.broadcasted_iota(jnp.int32, (8, 1), 0)
    lam = jnp.zeros((8, 1), F32)
    for h in range(heads):
        lam = jnp.where(map_row == h, lam_ref[h], lam)
    hgain = jnp.concatenate([hgain_ref[...]] * heads, axis=-1)

    def attention(g):
        if g:
            arrived(kbuf.at[pl.ds(g * GROUP, GROUP)], ksem.at[g])
            start_all(fetch_values, g + 1)
        else:
            arrived(kbuf.at[pl.ds(0, GROUP // 2)], ksem.at[pieces])
        for j in range(GROUP):
            s = g * GROUP + j
            if s == GROUP // 2:
                arrived(kbuf.at[pl.ds(s, GROUP // 2)], ksem.at[0])
                start_all(fetch_keys, 1)
            raw[j] = lax.dot_general(
                queries[s].astype(BF16), kbuf[s], (((1,), (1,)), ((), ())), preferred_element_type=F32
            )
        own_ws = []
        for j in range(GROUP):
            s = g * GROUP + j
            own = jnp.sum(queries[s] * own_keys[pl.ds(s, 1), :], axis=-1, keepdims=True) * scale
            scores = jnp.where(position < lengths_ref[s], raw[j] * scale, -jnp.inf)
            highest = jnp.maximum(jnp.max(scores, axis=-1, keepdims=True), own)
            raised = jnp.exp(scores - highest)
            own_raised = jnp.exp(own - highest)
            total = jnp.sum(raised, axis=-1, keepdims=True) + own_raised
            inv = 1.0 / total
            probs = raised * inv
            own_probs = own_raised * inv
            weights_v[j] = (probs - lam * pltpu.roll(probs, 4, 0)).astype(BF16)
            own_b = jnp.broadcast_to(own_probs, (8, 128))
            own_ws.append((own_b - lam * pltpu.roll(own_b, 4, 0)).astype(BF16).astype(F32)[:, :1])
        arrived(vbuf.at[pl.ds(g * GROUP, GROUP)], vsem.at[g])
        if g == 0:
            start_all(fetch_values, 1)
        start_all(fetch_keys, g + 2)
        outs = [
            jnp.dot(weights_v[j], vbuf[g * GROUP + j], preferred_element_type=F32) for j in range(GROUP)
        ]
        for j in range(GROUP):
            s = g * GROUP + j
            out = outs[j] + own_ws[j] * new_values[pl.ds(s, 1), :]
            out = jnp.where(mine, out, 0.0)
            mean_sq = jnp.sum(out * out, axis=-1, keepdims=True) * (1.0 / head)
            out = out * lax.rsqrt(mean_sq + EPS)
            attended[pl.ds(s, 1), :] = jnp.sum(out, axis=0, keepdims=True) * hgain

    def send_partials(g):
        heads_out = attended[g * GROUP:(g + 1) * GROUP, :].astype(BF16)
        partial = jnp.dot(heads_out, ow_v[...], preferred_element_type=F32)
        for q in range(parts):
            cut = partial[:, q * columns:(q + 1) * columns]
            part_f[q] = cut
            part_b[g, q] = cut.astype(BF16)
        for k in range(1, parts):
            peer = lax.rem(t + k, parts)
            send(part_b.at[g, peer], rs_buf.at[g, k - 1], 0, rs_r.at[g], (e, peer))
        kept[g] = kept[g] + part_f[t]

    own, last = {}, pieces - 1
    opposite = lax.rem(twin + 2, parts)

    def send_rows(g):
        arrived(rs_buf.at[g], rs_r.at[g])
        total = kept[g]
        for k in range(1, parts):
            total = total + rs_buf[g, k - 1].astype(F32)
        kept[g] = total
        xbuf[g, t, e] = (total * fgain).astype(BF16)
        view = xbuf.at[g, t, e]
        for m in range(groups - 1, 0, -1):
            for side in (t, across):
                send(view, view, 2, wide_r.at[g], (flip(e, m), side))
        own[g] = send(view, view, 3, own_r.at[g], (e, across))

    def join_rows(g):
        own[g].wait_recv()
        arrived(xbuf.at[g, pl.ds(0, 2), pl.ds(0, groups - 1)], wide_r.at[g])
        for side in (t, across):
            view = xbuf.at[g, side]
            send(view, view, 6, join_r.at[g], (e, twin))

    for g in range(pieces):
        attention(g)
        if g == 0:
            pl.semaphore_wait(barrier, parts - 1 + 2 * (groups - 1))
            loads[5].wait()
        send_partials(g)
        if g == 0:
            for m in range(groups - 1, 0, -1):
                send(slot_buf.at[e], slot_buf.at[e], 1, sl_r.at[0], (flip(e, m), t))
        if g >= 1:
            send_rows(g - 1)

    fetches = loads[6:]
    third = owned
    for load in fetches[:third]:
        load.start()
    arrived(slot_buf.at[pl.ds(0, groups - 1)], sl_r.at[0])
    base = e * block
    local = (where_is((block, n), 0) + base).astype(F32)
    chosen = [(slot_buf[b][:1, :] == local).astype(BF16) for b in range(groups)]

    def dispatch_from(first, count):
        wide_n = count * groups * GROUP
        token = where_is((n, wide_n), 0) // top
        spot_row = (token // GROUP - first) * (groups * GROUP) + token % GROUP
        place = []
        for b in range(groups):
            spot = (where_is((n, wide_n), 1) == spot_row + b * GROUP).astype(BF16)
            placed = jnp.dot(chosen[b], spot, preferred_element_type=F32)
            place.append(placed.reshape(owned, 1, capacity, wide_n))
        return jnp.concatenate(place, axis=1).reshape(groups * block, wide_n).astype(BF16)

    def rows_from(first, count, q):
        rows = xbuf[first:first + count, q].astype(F32)
        return rows.reshape(count * groups * GROUP, columns).astype(BF16)

    _, later = route_tables(routes_ref[...], logits_ref[...], groups * block, capacity)
    share = later()
    for i in range(3):
        coarse = share.astype(BF16)
        combine_v[i * seqs:(i + 1) * seqs, :] = coarse
        share = share - coarse.astype(F32)
    dispatch_first = dispatch_from(0, last)
    dispatch_v[...] = dispatch_from(last, 1)
    send_rows(last)
    for load in fetches[third:]:
        load.start()
    for g in range(last):
        join_rows(g)
    for g in range(last):
        arrived(xbuf.at[g, pl.ds(0, 2)], join_r.at[g])
    for q in range(parts):
        lines_v[:, q * columns:(q + 1) * columns] = jnp.dot(
            dispatch_first, rows_from(0, last, q), preferred_element_type=F32
        )
    join_rows(last)

    def partial_hidden(j, sides):
        rated, gate, up = jnp.zeros((per, columns), F32), jnp.zeros((per, deep), F32), jnp.zeros((per, deep), F32)
        for q in sides:
            cut = pl.ds(pl.multiple_of(q * columns, columns), columns)
            late = xbuf[last, q].astype(F32).reshape(groups * GROUP, columns).astype(BF16)
            picked = jnp.dot(dispatch_v[j * per:(j + 1) * per, :], late, preferred_element_type=F32)
            picked = picked + lines_v[j * per:(j + 1) * per, cut]
            line = picked.astype(BF16)
            gate += jnp.dot(line, gate_v[j, cut, :], preferred_element_type=F32)
            up += jnp.dot(line, up_v[j, cut, :], preferred_element_type=F32)
            plain = picked * (1.0 / fgain_ref[:, cut])
            rated = rated + plain * plain
        return jnp.sum(rated, axis=-1, keepdims=True), gate, up

    deep = hbuf.shape[3]
    ahead = 2
    for j in range(owned):
        for i in range(2):
            loads[6 + 3 * j + i].wait()
    for j in range(ahead):
        squares, gate, up = partial_hidden(j, (t, across))
        squares_v[j] = jnp.broadcast_to(squares, (per, 128))
        gate_up[j, 0], gate_up[j, 1] = gate, up
    arrived(xbuf.at[last, pl.ds(0, 2)], join_r.at[last])
    hfar, hnear = [None], [None]
    half_rows = groups // 2 * capacity
    home = e // (groups // 2) * (groups // 2)
    away = groups // 2 - home
    for j in range(owned):
        if j < ahead:
            squares, gate, up = partial_hidden(j, (twin, opposite))
            squares = squares + squares_v[j][:, :1]
            gate, up = gate + gate_up[j, 0], up + gate_up[j, 1]
        else:
            squares, gate, up = partial_hidden(j, (t, across, twin, opposite))
        line_scale = lax.rsqrt(squares * (1.0 / (columns * parts)) + EPS)
        gate = jnp.minimum(gate * line_scale, LIMIT)
        up = jnp.clip(up * line_scale, -LIMIT, LIMIT)
        hbuf[j, t] = ((up + 1.0) * gate * jax.nn.sigmoid(ALPHA * gate)).astype(BF16)
        if j == 0:
            halves = []
            for i, base_row in enumerate((away, home)):
                view = hbuf.at[j, t, pl.ds(pl.multiple_of(base_row * capacity, half_rows), half_rows)]
                halves.append([
                    send(view, view, 4, hy_r.at[i * owned], (e, across)),
                    send(view, view, 4, hd_r.at[i * owned], (e, opposite)),
                    send(view, view, 4, hc_r.at[i * owned], (e, twin)),
                ])
            continue
        view = hbuf.at[j, t]
        hfar.append(send(view, view, 4, hy_r.at[j], (e, across)))
        hnear.append(send(view, view, 4, hc_r.at[j], (e, twin)))
    hrelay = [None]
    loads[6 + 2].wait()
    for i, base_row in enumerate((away, home)):
        for copy in halves[i]:
            copy.wait_recv()
        result = jnp.zeros((half_rows, columns), F32)
        cut = pl.ds(pl.multiple_of(base_row * capacity, half_rows), half_rows)
        for q in range(parts):
            result += jnp.dot(hbuf[0, q, cut, :], down_v[0, q * deep:(q + 1) * deep, :], preferred_element_type=F32)
        resbuf[0, pl.ds(base_row, groups // 2)] = result.reshape(groups // 2, capacity, columns).astype(BF16)
        for m in (range(groups - 1, groups // 2 - 1, -1) if i == 0 else range(groups // 2 - 1, 0, -1)):
            peer = flip(e, m)
            send(resbuf.at[0, peer], ret.at[e, 0], 5, re_r.at[0], (peer, t))
    ret[e, 0] = resbuf[0, e]
    for j in range(1, owned + 1):
        if j < owned:
            hfar[j].wait_recv()
            theirs = hbuf.at[j, across]
            hrelay.append(send(theirs, theirs, 4, hd_r.at[j], (e, twin)))
        if j == 1:
            continue
        i = j - 1
        hnear[i].wait_recv()
        hrelay[i].wait_recv()
        loads[6 + 3 * i + 2].wait()
        result = jnp.zeros((per, columns), F32)
        for q in range(parts):
            result += jnp.dot(hbuf[i, q], down_v[i, q * deep:(q + 1) * deep, :], preferred_element_type=F32)
        resbuf[i] = result.reshape(groups, capacity, columns).astype(BF16)
        for m in range(groups - 1, 0, -1):
            peer = flip(e, m)
            send(resbuf.at[i, peer], ret.at[e, i], 5, re_r.at[0], (peer, t))
        ret[e, i] = resbuf[i, e]
    arrived(ret.at[pl.ds(0, groups - 1)], re_r.at[0])
    results = ret[...].astype(F32).reshape(groups * block, columns).astype(BF16)
    moe = jnp.dot(combine_v[...], results, preferred_element_type=F32)
    moe = moe[:seqs] + moe[seqs:2 * seqs] + moe[2 * seqs:]
    out_ref[...] = (kept[...].reshape(seqs, columns) + moe).astype(out_ref.dtype)
    arrived(part_b.at[:, pl.ds(0, parts - 1)], snd.at[0])
    arrived(slot_buf.at[pl.ds(0, groups - 1)], snd.at[1])
    arrived(xbuf.at[:, pl.ds(0, 2), pl.ds(0, groups - 1)], snd.at[2])
    arrived(xbuf.at[:, 0, 0], snd.at[3])
    arrived(xbuf.at[:, pl.ds(0, 2)], snd.at[6])
    arrived(hbuf.at[:, pl.ds(0, parts - 1)], snd.at[4])
    arrived(resbuf.at[:, pl.ds(0, groups - 1)], snd.at[5])


def layer(
    tokens, lengths, cache_keys, cache_values, attn_gain, q1w, q2w, k1w, k2w, vw, lam, hgain, out_w,
    ffn_gain, routes, logits, gate_w, up_w, down_w, groups, parts, capacity,
):
    seqs, length, width = cache_keys.shape
    heads = lam.shape[0]
    owned, _, deep = gate_w.shape
    columns = down_w.shape[2]
    per = groups * capacity
    pieces = seqs // GROUP
    full = tokens.shape[1]
    routes, logits = routes.T, logits.T
    anyspace = pl.BlockSpec(memory_space=pltpu.HBM)
    scratch = [pltpu.VMEM(cache_keys.shape, BF16), pltpu.VMEM(cache_values.shape, BF16)]
    scratch += [pltpu.VMEM(w.shape, BF16) for w in (q1w, q2w, k1w, k2w, vw, out_w, gate_w, up_w, down_w)]
    scratch += [
        pltpu.VMEM((seqs, 8, width), F32),
        pltpu.VMEM((seqs, width), F32),
        pltpu.VMEM((seqs, width), F32),
        pltpu.VMEM((seqs, width), F32),
        pltpu.VMEM((GROUP, 8, length), F32),
        pltpu.VMEM((GROUP, 8, length), BF16),
        pltpu.SMEM(lam.shape, F32),
        pltpu.SMEM((seqs,), jnp.int32),
        pltpu.VMEM(tokens.shape, BF16),
        pltpu.VMEM((1, full), F32),
        pltpu.VMEM((1, hgain.shape[0]), F32),
        pltpu.VMEM((1, full), F32),
        pltpu.VMEM(routes.shape, routes.dtype),
        pltpu.VMEM(logits.shape, F32),
        pltpu.VMEM(tokens.shape, F32),
        pltpu.VMEM((parts, GROUP, columns), F32),
        pltpu.VMEM((pieces, parts, GROUP, columns), BF16),
        pltpu.VMEM((pieces, parts - 1, GROUP, columns), BF16),
        pltpu.VMEM((pieces, GROUP, columns), F32),
        pltpu.VMEM((groups, 8, routes.size), F32),
        pltpu.VMEM((3 * seqs, owned * per), BF16),
        pltpu.VMEM((owned * per, groups * GROUP), BF16),
        pltpu.VMEM((owned * per, full), F32),
        pltpu.VMEM((owned, per, 128), F32),
        pltpu.VMEM((owned, 2, per, deep), F32),
        pltpu.VMEM((pieces, parts, groups, GROUP, columns), BF16),
        pltpu.VMEM((owned, parts, per, deep), BF16),
        pltpu.VMEM((owned, groups, capacity, columns), BF16),
        pltpu.VMEM((groups, owned, capacity, columns), BF16),
    ]
    dma = lambda *shape: [pltpu.SemaphoreType.DMA(shape)]
    scratch += dma(pieces + 1) * 2 + dma(6 + 3 * owned) + dma(8)
    scratch += dma(7) + dma(pieces) + dma(1) + dma(pieces) * 3 + dma(owned + 1) * 3 + dma(1)
    return pl.pallas_call(
        functools.partial(layer_kernel, heads, groups, parts, capacity),
        out_shape=pltpu.VMEM((seqs, columns), BF16),
        in_specs=[anyspace] * 19,
        out_specs=pl.BlockSpec(memory_space=pltpu.VMEM),
        scratch_shapes=scratch,
        compiler_params=pltpu.CompilerParams(
            collective_id=0, has_side_effects=True, vmem_limit_bytes=LAYER_BYTES
        ),
        name="layer",
    )(
        lam, lengths, tokens, attn_gain.reshape(1, -1), hgain.reshape(1, -1), ffn_gain.reshape(1, -1),
        routes, logits, cache_keys, cache_values, q1w, q2w, k1w, k2w, vw, out_w, gate_w, up_w, down_w,
    )


def slot_tables(routes, weights, expert_ids, capacity):
    blocks, seqs, top = routes.shape
    flat = routes.reshape(blocks, seqs * top)
    order = jnp.arange(seqs * top, dtype=jnp.int32)
    same = (flat[:, None, :] == flat[:, :, None]) & (order[None, None, :] < order[None, :, None])
    rank = jnp.sum(same.astype(jnp.int32), axis=2)
    match = flat[:, :, None] == expert_ids[None, None, :]
    hit = rank[:, :, None] == jnp.arange(capacity, dtype=jnp.int32)[None, None, :]
    table = (match[:, :, :, None] & hit[:, :, None, :]).astype(jnp.float32)
    table = table.reshape(blocks, seqs, top, expert_ids.shape[0], capacity)
    dispatch = jnp.sum(table, axis=2)
    combine = jnp.sum(table * weights[:, :, :, None, None], axis=2)
    return (dispatch, combine)


def run_experts(buffer, gate_w, up_w, down_w):
    gate = jnp.einsum("bjcd,jdf->bjcf", buffer, gate_w, preferred_element_type=jnp.float32)
    up = jnp.einsum("bjcd,jdf->bjcf", buffer, up_w, preferred_element_type=jnp.float32)
    bound_gate = jnp.minimum(gate, LIMIT)
    bound_up = jnp.clip(up, -LIMIT, LIMIT)
    hidden = ((bound_up + 1.0) * bound_gate * jax.nn.sigmoid(ALPHA * bound_gate)).astype(
        jnp.bfloat16
    )
    total = jnp.einsum(
        "bjcf,jfd->bjcd",
        lax.all_gather(hidden, "tp", axis=3, tiled=True),
        down_w,
        preferred_element_type=jnp.float32,
    )
    return total.astype(jnp.bfloat16)


def per_device(
    tokens,
    lengths,
    cache_keys,
    cache_values,
    attn_gain,
    q_first_w,
    q_second_w,
    k_first_w,
    k_second_w,
    value_w,
    mix_lambda,
    head_gain,
    out_w,
    ffn_gain,
    routes,
    route_logits,
    gate_w,
    up_w,
    down_w,
):
    groups, parts = lax.axis_size("ep"), lax.axis_size("tp")
    owned = gate_w.shape[0]
    seqs, top = routes.shape
    capacity = max(2, 2 * seqs * top // (owned * groups))
    fused = (
        parts == 4 and seqs % GROUP == 0 and seqs >= 4 * GROUP and capacity % 8 == 0 and seqs * top % 128 == 0 and groups & (groups - 1) == 0
    )
    if fused:
        return layer(
            tokens, lengths, cache_keys, cache_values, attn_gain, q_first_w, q_second_w, k_first_w, k_second_w,
            value_w, mix_lambda, head_gain, out_w, ffn_gain, routes, route_logits, gate_w, up_w, down_w,
            groups, parts, capacity,
        )
    partial_value = attend(
        tokens,
        lengths,
        cache_keys,
        cache_values,
        attn_gain,
        q_first_w,
        q_second_w,
        k_first_w,
        k_second_w,
        value_w,
        mix_lambda,
        head_gain,
        out_w,
        F32,
        1,
    )
    partial_value = partial_value.reshape(tokens.shape)
    wide = tokens.astype(F32)
    columns = wide.shape[1] // lax.axis_size("tp")
    start = lax.axis_index("tp") * columns
    summed = lax.psum(partial_value, "tp")
    after = wide + summed
    full_in = rms_scale(after, ffn_gain).astype(jnp.bfloat16)
    kept = lax.dynamic_slice_in_dim(after, start, columns, 1)
    weights = jax.nn.softmax(route_logits, axis=-1)
    expert_ids = jnp.arange(owned * groups, dtype=jnp.int32)
    dispatch, combine = slot_tables(routes[None], weights[None], expert_ids, capacity)
    buffer = jnp.einsum(
        "bsjc,bsd->bjcd",
        dispatch.astype(jnp.bfloat16),
        full_in[None],
        preferred_element_type=jnp.float32,
    ).astype(jnp.bfloat16)
    buffer = buffer.reshape(groups, owned, capacity, -1)
    arrived = lax.all_to_all(buffer, "ep", split_axis=0, concat_axis=0, tiled=True)
    results = run_experts(arrived, gate_w, up_w, down_w)
    returned = lax.all_to_all(results, "ep", split_axis=0, concat_axis=0, tiled=True).reshape(
        1, groups * owned, capacity, -1
    )
    moe = jnp.einsum(
        "bsjc,bjcd->bsd", combine, returned.astype(jnp.float32), precision=lax.Precision.HIGHEST
    )[0]
    return (kept + moe).astype(jnp.bfloat16)


def solution(mesh):
    return jax.shard_map(
        per_device,
        mesh=mesh,
        in_specs=(
            P("ep", None),
            P("ep"),
            P("ep", None, "tp"),
            P("ep", None, "tp"),
            P(),
            P(None, "tp"),
            P(None, "tp"),
            P(None, "tp"),
            P(None, "tp"),
            P(None, "tp"),
            P("tp"),
            P(),
            P("tp", None),
            P(),
            P("ep", None),
            P("ep", None),
            P("ep", None, "tp"),
            P("ep", None, "tp"),
            P("ep", None, "tp"),
        ),
        out_specs=P("ep", "tp"),
        check_vma=False,
    )
```
